32 devices in a mesh: sp: 8 (over z, x), tp: 4 (over y, core).
Axes of the slice: x: 2, y: 2, z: 4, core: 2. Of those that a mesh axis runs over, the one named last changes fastest.
Arguments:
- pool_input: bfloat16 [1024, 1024], P('sp', 'tp'), may hold values from -12 to 12
- doc_ids: int32 [1024], P('sp'), may hold values from 0 to 1, as said below
- residual: bfloat16 [1024, 2048], P('sp', 'tp'), may hold values from -30 to 30
- pool_gain: float32 [1024], P('tp'), may hold values from 0.1 to 1.9
- out_proj: bfloat16 [1024, 2048], P('tp'), may hold values from -0.25 to 0.25
- norm_gain: float32 [2048], P('tp'), may hold values from 0.1 to 1.9
- routes: int32 [1024, 2], P('sp'), may hold values from 0 to 7, all different within a row; in each aligned block of 128 rows (0 to 127, 128 to 255, ...) at most 64 rows name the same one
- route_weights: float32 [1024, 2], P('sp'), may hold values from 0.2 to 1.2
- expert_gate: bfloat16 [8, 2048, 4096], P('sp', None, 'tp'), may hold values from -0.125 to 0.125
- expert_up: bfloat16 [8, 2048, 4096], P('sp', None, 'tp'), may hold values from -0.125 to 0.125
- expert_down: bfloat16 [8, 4096, 2048], P('sp', 'tp'), may hold values from -0.125 to 0.125
- shared_gate: bfloat16 [2048, 1024], P(None, 'tp'), may hold values from -0.125 to 0.125
- shared_up: bfloat16 [2048, 1024], P(None, 'tp'), may hold values from -0.125 to 0.125
- shared_down: bfloat16 [1024, 2048], P('tp'), may hold values from -0.25 to 0.25
Outputs:
- layer_out: bfloat16 [1024, 2048], P('sp', 'tp')
The draws below stay inside these ranges and needn't reach their ends.
Inputs may be any that keep to these rules, and one draw needn't show every extreme that they name: `routes`: each row names 2 different experts. In each aligned block of 128 rows no expert is named by more than 64 rows; in some blocks one expert is named by exactly 64 rows. `doc_ids`: document numbers start at 0, never fall along the sequence and rise by one at each document's start.
All inputs are finite; a program needn't handle non-finite values.
Results may differ from the reference program's by a relative error of at most 0.015.
Values may be sent and summed in bfloat16 or wider, within the bound.
A program may use at most 64 MiB of HBM per device.

```python
import math
import jax
import jax.numpy as jnp
import numpy as np
from jax import lax

D = 2048
PW = 1024
FF_E = 4096
FF_S = 1024
TOP_K = 2
TOK_DEV = 128
TOKENS = 1024
EXPERTS = 8
CAP = 64
N_SP = 8
N_TP = 4


def draw_doc_ids(key, part):
    documents = max(2, N_SP // 4)
    spacing = TOKENS // documents
    offsets = jax.random.randint(jax.random.fold_in(key, 31), (documents - 1,), TOK_DEV // 4, 3 * TOK_DEV // 4 + 1)
    starts = jnp.arange(1, documents, dtype=jnp.int32) * spacing + offsets.astype(jnp.int32)
    positions = jnp.arange(TOKENS, dtype=jnp.int32)
    return jnp.sum((positions[:, None] >= starts[None, :]).astype(jnp.int32), axis=1).astype(jnp.int32)


def draw_pool_input(key, part):
    noise_key, level_key = jax.random.split(jax.random.fold_in(key, 11))
    levels = jax.random.normal(level_key, (TOKENS // 16, PW), jnp.float32)
    levels = jnp.repeat(levels, 16, axis=0)
    noise = jax.random.normal(noise_key, (TOKENS, PW), jnp.float32)
    values = noise + 1.5 * levels
    return jnp.clip(values, -12.0, 12.0).astype(jnp.bfloat16)


def draw_residual(key, part):
    noise_key, column_key = jax.random.split(jax.random.fold_in(key, 23))
    position = jnp.arange(D, dtype=jnp.float32) / (D - 1)
    noise = jax.random.normal(noise_key, (TOKENS, D), jnp.float32)
    scales = jnp.exp(jnp.log(3.0) * position + jax.random.uniform(column_key, (D,), jnp.float32, -0.5, 0.5))
    return jnp.clip(noise * scales[None, :], -30.0, 30.0).astype(jnp.bfloat16)


def strengthened(array, rng, source, target, shards_of, factor):
    def block_of(dim):
        return (jnp.arange(array.shape[dim]) // (array.shape[dim] // shards_of)).reshape((-1,) + (1,) * (array.ndim - 1 - dim))

    one_side = jax.random.permutation(rng, shards_of)[block_of(target)]
    far = (block_of(target) + shards_of // 2) % shards_of
    return jnp.where((block_of(source) == one_side) | (block_of(source) == far), factor * array, array)


def block_scale(rng, extent, cuts, least, high):
    level = 1.0
    for dim, parts in cuts:
        draws = jax.random.uniform(jax.random.fold_in(jax.random.fold_in(rng, 6), dim), (parts,), jnp.float32, least / len(cuts), high / len(cuts))
        level = level * jnp.repeat(jnp.exp(draws), extent[dim] // parts).reshape((-1,) + (1,) * (len(extent) - 1 - dim))
    return level


def assign_block(rng, own, number, rows, number_of, top, reach, skew):
    ranking = jax.random.permutation(rng, number_of)
    crowded, usual = portions_of(number_of, rows * top, reach, skew, True), portions_of(number_of, rows * top, reach, skew, False)
    places = jnp.arange(number_of)

    def named(lengths, turn):
        used = int((lengths > 0).sum())
        fixed = max(1, used // 4)
        passed = fixed + (places - fixed + turn * (used - fixed)) % max(1, number_of - fixed)
        return jnp.zeros((number_of,), jnp.int32).at[ranking[jnp.where(places < fixed, places, passed)]].set(jnp.asarray(lengths, jnp.int32))

    lengths = jnp.where(number % 4 == 0, named(crowded, number // 4), named(usual, number - number // 4 - 1))
    mixed = jax.random.permutation(jax.random.fold_in(own, 3), number_of)
    source_of, receiver = mixed[0:number_of // 2 * 2:2], mixed[1:number_of // 2 * 2:2]
    room = jnp.minimum(lengths[source_of] - 1, reach - lengths[receiver]) // 2
    room = jnp.where((source_of == ranking[0]) | (receiver == ranking[0]) | (lengths[receiver] == 0), 0, jnp.maximum(room, 0))
    passed = jax.random.randint(jax.random.fold_in(own, 4), (number_of // 2,), 0, 1 << 20) % (room + 1)
    lengths = lengths.at[source_of].add(-passed).at[receiver].add(passed)
    labels = jnp.searchsorted(jnp.cumsum(lengths), jnp.arange(rows * top), side="right").astype(jnp.int32)
    grid = labels.reshape(top, rows).T
    grid = grid[jax.random.permutation(jax.random.fold_in(own, 1), rows)]
    turn = jax.random.randint(jax.random.fold_in(own, 2), (rows, 1), 0, top)
    return jnp.take_along_axis(grid, (jnp.arange(top)[None, :] + turn) % top, axis=1)


def portions_of(count, total, limit, slope, full):
    loads = [(1 << 20) // math.isqrt(rank ** slope) + 1 for rank in range(1, count + 1)]
    largest = limit if full else min(limit, max(-(-total // count), total * loads[0] // sum(loads)))
    least = 1 if total - largest >= count - 1 else 0
    holding, spare = [largest] + [least] * (count - 1), total - largest - least * (count - 1)
    while spare > 0:
        movable = [i for i in range(1, count) if holding[i] < largest] or [i for i in range(1, count) if holding[i] < limit]
        mass, left = sum([loads[i] for i in movable]), spare
        for i in movable:
            extra = min(limit - holding[i], max(1, left * loads[i] // mass), spare)
            holding[i] = holding[i] + extra
            spare = spare - extra
    return np.array(holding)


def centred(key, dims, spread, limit, cuts=(), kind=jnp.bfloat16):
    drawn = jax.random.normal(key, dims, jnp.float32) * spread
    if len(cuts) > 0:
        drawn = block_scale(key, dims, cuts, -0.22, 0.18) * drawn
    return jnp.clip(drawn, min=-limit, max=limit).astype(kind)


def bell_draw_with(key, extent, spread, most, cuts, heavy, kind=jnp.bfloat16):
    values = spread * jax.random.normal(key, extent, jnp.float32)
    if cuts:
        values = values * block_scale(key, extent, cuts, -0.22, 0.18)
    return jnp.clip(strengthened(values, jax.random.fold_in(key, 3), *heavy), -most, most).astype(kind)


def setup_inputs(seed: int = 0) -> dict:
    arg_keys = jax.random.split(jax.random.key(seed), 15)
    pool_input = draw_pool_input(jax.random.fold_in(arg_keys[14], 71), 0)
    doc_ids = draw_doc_ids(jax.random.fold_in(arg_keys[14], 71), 0)
    residual = draw_residual(jax.random.fold_in(arg_keys[14], 71), 0)
    pool_gain = jnp.clip(1.0 + 0.18 * jax.random.normal(arg_keys[3], (PW,), jnp.float32), 0.1, 1.9)
    out_proj = bell_draw_with(arg_keys[4], (PW, D), PW ** -0.5, 0.25, ((0, 4),), (0, 1, 4, 2.0))
    norm_gain = jnp.clip(1.0 + 0.18 * jax.random.normal(arg_keys[5], (D,), jnp.float32), 0.1, 1.9)
    routes_keys = jax.random.split(jax.random.fold_in(arg_keys[6], 1), TOKENS // TOK_DEV)
    routes_turns = jax.random.permutation(jax.random.fold_in(arg_keys[6], 3), TOKENS // TOK_DEV)
    routes = jax.vmap(lambda own, number: assign_block(jax.random.fold_in(arg_keys[6], 2), own, number, TOK_DEV, EXPERTS, TOP_K, CAP, 1))(routes_keys, routes_turns).reshape((TOKENS, TOP_K))
    route_weights = jnp.clip(jnp.exp(math.log(1.2) - 1.7917595 * jax.random.uniform(arg_keys[7], (TOKENS, TOP_K), jnp.float32) ** block_scale(arg_keys[7], (TOKENS, TOP_K), ((0, 8),), -0.2, 0.2)), 0.2, 1.2)
    expert_gate = centred(arg_keys[8], (EXPERTS, D, FF_E), D ** -0.5, 0.125, ((0, 8), (2, 4)))
    expert_up = centred(arg_keys[9], (EXPERTS, D, FF_E), D ** -0.5, 0.125, ((0, 8), (2, 4)))
    expert_down = bell_draw_with(arg_keys[10], (EXPERTS, FF_E, D), FF_E ** -0.5, 0.125, ((0, 8), (1, 4)), (1, 2, 4, 2.0))
    shared_gate = centred(arg_keys[11], (D, FF_S), D ** -0.5, 0.125, ((1, 4),))
    shared_up = centred(arg_keys[12], (D, FF_S), D ** -0.5, 0.125, ((1, 4),))
    shared_down = bell_draw_with(arg_keys[13], (FF_S, D), FF_S ** -0.5, 0.25, ((0, 4),), (0, 1, 4, 2.0))
    return {"pool_input": pool_input, "doc_ids": doc_ids, "residual": residual, "pool_gain": pool_gain, "out_proj": out_proj, "norm_gain": norm_gain, "routes": routes, "route_weights": route_weights, "expert_gate": expert_gate, "expert_up": expert_up, "expert_down": expert_down, "shared_gate": shared_gate, "shared_up": shared_up, "shared_down": shared_down}


def blocked_down(hidden, down_weight, groups):
    width = hidden.shape[1] // groups
    pieces = jnp.moveaxis(hidden.reshape(hidden.shape[0], groups, width), 1, 0)
    weights = down_weight.reshape(groups, width, down_weight.shape[1])

    def add_group(accumulated, pair):
        product = jnp.dot(pair[0], pair[1], preferred_element_type=jnp.float32)
        rounded = lax.optimization_barrier(product.astype(jnp.bfloat16))
        return (accumulated + rounded.astype(jnp.float32), None)
    initial = jnp.zeros((hidden.shape[0], down_weight.shape[1]), jnp.float32)
    summed, unused = lax.scan(add_group, initial, (pieces, weights))
    return summed.astype(jnp.bfloat16)

def reference(pool_input, doc_ids, residual, pool_gain, out_proj, norm_gain, routes, route_weights, expert_gate, expert_up, expert_down, shared_gate, shared_up, shared_down):
    values = pool_input.astype(jnp.float32)
    positions = jnp.arange(TOKENS, dtype=jnp.int32)
    begins = jnp.concatenate([jnp.ones((1,), bool), doc_ids[1:] != doc_ids[:-1]])
    doc_start = lax.cummax(jnp.where(begins, positions, 0), axis=0)
    length = (positions - doc_start + 1).astype(jnp.float32)
    scale_index = jnp.arange(PW, dtype=jnp.int32) % 4
    window_size = jnp.where(scale_index == 0, 2.0, jnp.where(scale_index == 1, 8.0, 16.0))
    padded = jnp.concatenate([jnp.zeros((15, PW), jnp.float32), values], 0)
    window_total = jnp.zeros((TOKENS, PW), jnp.float32)
    for offset in range(16):
        inside = (offset < length[:, None]) & (offset < window_size[None, :])
        window_total = window_total + jnp.where(inside, padded[15 - offset:15 - offset + TOKENS], 0.0)
    window_mean = window_total / jnp.minimum(length[:, None], window_size[None, :])
    running = jnp.cumsum(values[:, 3::4], axis=0)
    shifted = jnp.concatenate([jnp.zeros((1, PW // 4), jnp.float32), running], 0)
    doc_sum = running - jnp.take(shifted, doc_start, axis=0)
    doc_mean = doc_sum / length[:, None]
    pool_mean = jnp.concatenate([window_mean.reshape(TOKENS, PW // 4, 4)[..., :3], doc_mean[..., None]], -1)
    pool_mean = pool_mean.reshape(TOKENS, PW)
    pooled = ((pool_mean - values) * pool_gain).astype(jnp.bfloat16)
    projected = blocked_down(pooled, out_proj, N_TP)
    hidden_state = residual.astype(jnp.float32) + projected.astype(jnp.float32)
    squares = lax.optimization_barrier(jnp.mean(hidden_state * hidden_state, axis=1, keepdims=True))
    normed = (hidden_state * lax.rsqrt(squares + 1e-06) * norm_gain).astype(jnp.bfloat16)
    flat_experts = routes.reshape(N_SP, TOK_DEV * TOP_K)
    onehot = (flat_experts[..., None] == jnp.arange(EXPERTS, dtype=jnp.int32)).astype(jnp.int32)
    ranks = lax.optimization_barrier(jnp.sum((jnp.cumsum(onehot, axis=1) - 1) * onehot, axis=2))
    block_ids = jnp.arange(N_SP, dtype=jnp.int32)[:, None]
    slot_index = ((flat_experts * N_SP + block_ids) * CAP + ranks).reshape(-1).astype(jnp.int32)
    token_index = (jnp.arange(TOKENS * TOP_K, dtype=jnp.int32) // TOP_K).astype(jnp.int32)
    table_rows = EXPERTS * N_SP * CAP
    slot_token = jnp.full((table_rows,), TOKENS, jnp.int32).at[slot_index].set(token_index)
    with_blank = jnp.concatenate([normed, jnp.zeros((1, D), jnp.bfloat16)], 0)
    expert_rows = jnp.take(with_blank, slot_token, axis=0).reshape(EXPERTS, N_SP * CAP, D)

    def run_expert(group):
        rows_in, gate_weight, up_weight, down_weight = group
        gate = jnp.dot(rows_in, gate_weight, preferred_element_type=jnp.float32)
        upper = jnp.dot(rows_in, up_weight, preferred_element_type=jnp.float32)
        hidden = (jax.nn.silu(gate) * upper).astype(jnp.bfloat16)
        return blocked_down(hidden, down_weight, N_TP)
    expert_out = lax.map(run_expert, (expert_rows, expert_gate, expert_up, expert_down)).reshape(table_rows, D)
    picked = jnp.take(expert_out, slot_index, axis=0).astype(jnp.float32) * route_weights.reshape(-1)[:, None]
    routed = lax.optimization_barrier(jnp.sum(picked.reshape(TOKENS, TOP_K, D), axis=1))
    shared_gate_out = jnp.dot(normed, shared_gate, preferred_element_type=jnp.float32)
    shared_up_out = jnp.dot(normed, shared_up, preferred_element_type=jnp.float32)
    shared_hidden = (jax.nn.silu(shared_gate_out) * shared_up_out).astype(jnp.bfloat16)
    shared_out = blocked_down(shared_hidden, shared_down, N_TP)
    return (hidden_state + routed + shared_out.astype(jnp.float32)).astype(jnp.bfloat16)
```

```python
import jax
import functools
import jax.numpy as jnp
from jax import lax
from jax.experimental import pallas as pl
from jax.experimental.pallas import tpu as pltpu
from jax.sharding import PartitionSpec as P


def carried_in(value, axis, join, neutral):
    count, mine = (lax.axis_size(axis), lax.axis_index(axis))
    pieces = jax.tree.map(lambda part: lax.all_gather(part, axis), value)
    subtotal = jax.tree.map(
        lambda part, zero: jnp.full_like(part, 0) + jnp.asarray(zero, part.dtype), value, neutral
    )

    def hop(position, subtotal):
        longer = join(subtotal, jax.tree.map(lambda part: part[position], pieces))
        return jax.tree.map(lambda new, old: jnp.where(position < mine, new, old), longer, subtotal)

    return lax.fori_loop(0, count - 1, hop, subtotal)


def from_behind(value, axis, by):
    size = lax.axis_size(axis)
    pairs = [(i, i + by) for i in range(size) if 0 <= i + by < size]
    return lax.ppermute(value, axis, pairs)


def join_documents(earlier, later):
    earlier_sum, earlier_length, earlier_first, earlier_last, earlier_inner = earlier
    later_sum, later_length, later_first, later_last, later_inner = later
    boundary = later_first != earlier_last
    restart = (later_inner > 0) | boundary
    merged = (
        jnp.where(restart, later_sum, earlier_sum + later_sum),
        jnp.where(restart, later_length, earlier_length + later_length),
        earlier_first,
        later_last,
        jnp.maximum(jnp.maximum(earlier_inner, later_inner), boundary.astype(jnp.float32)),
    )
    earlier_empty = earlier_first < 0
    later_empty = later_first < 0
    return tuple(
        (
            jnp.where(earlier_empty, second, jnp.where(later_empty, first_value, joined))
            for first_value, second, joined in zip(earlier, later, merged)
        )
    )


def expert_terms(arrived, gate_weight, up_weight, down_weight):
    local_experts = gate_weight.shape[0]
    sources = arrived.shape[0] // local_experts
    grouped = arrived.reshape(sources, local_experts, arrived.shape[1], arrived.shape[2])
    gate = jnp.einsum("secd,edf->secf", grouped, gate_weight, preferred_element_type=jnp.float32)
    upper = jnp.einsum("secd,edf->secf", grouped, up_weight, preferred_element_type=jnp.float32)
    hidden = (jax.nn.silu(gate) * upper).astype(jnp.bfloat16)
    output = jnp.einsum("secf,efd->secd", hidden, down_weight, preferred_element_type=jnp.float32)
    return output.reshape(arrived.shape[0], arrived.shape[1], down_weight.shape[2])


def plain_body(
    pool_input,
    doc_ids,
    residual,
    pool_gain,
    out_proj,
    norm_gain,
    routes,
    route_weights,
    expert_gate,
    expert_up,
    expert_down,
    shared_gate,
    shared_up,
    shared_down,
):
    row_count, channels = pool_input.shape
    values = pool_input.astype(jnp.float32)
    positions = jnp.arange(row_count, dtype=jnp.int32)
    inner_begin = jnp.concatenate([jnp.zeros((1,), bool), doc_ids[1:] != doc_ids[:-1]])
    running = jnp.cumsum(values[:, 3::4], axis=0)
    shifted = jnp.concatenate([jnp.zeros((1, running.shape[1]), jnp.float32), running], 0)
    inner_last = jnp.max(jnp.where(inner_begin, positions, 0))
    own_terms = (
        running[-1] - shifted[inner_last],
        (row_count - inner_last).astype(jnp.float32),
        doc_ids[0].astype(jnp.float32),
        doc_ids[-1].astype(jnp.float32),
        jnp.any(inner_begin).astype(jnp.float32),
    )
    identity = (
        jnp.zeros((running.shape[1],), jnp.float32),
        jnp.zeros((), jnp.float32),
        jnp.full((), -1.0, jnp.float32),
        jnp.full((), -1.0, jnp.float32),
        jnp.zeros((), jnp.float32),
    )
    before = carried_in(own_terms, "sp", join_documents, identity)
    fresh = (before[2] < 0) | (doc_ids[0].astype(jnp.float32) != before[3])
    begins = jnp.concatenate([fresh[None], inner_begin[1:]])
    doc_start = lax.cummax(jnp.where(begins, positions, -1), axis=0)
    found = doc_start >= 0
    carry_sum = jnp.where(fresh, 0.0, before[0])
    carry_length = jnp.where(fresh, 0.0, before[1])
    length = jnp.where(
        found,
        (positions - doc_start + 1).astype(jnp.float32),
        carry_length + (positions + 1).astype(jnp.float32),
    )
    start_rows = jnp.take(shifted, jnp.maximum(doc_start, 0), axis=0)
    doc_sum = jnp.where(found[:, None], running - start_rows, carry_sum[None, :] + running)
    doc_mean = doc_sum / length[:, None]
    rim = from_behind(pool_input[row_count - 15 :], "sp", 1)
    extended = jnp.concatenate([rim, pool_input], 0).astype(jnp.float32)
    scale_index = jnp.arange(channels, dtype=jnp.int32) % 4
    window_size = jnp.where(scale_index == 0, 2.0, jnp.where(scale_index == 1, 8.0, 16.0))
    window_total = jnp.zeros((row_count, channels), jnp.float32)
    for offset in range(16):
        inside = (offset < length[:, None]) & (offset < window_size[None, :])
        window_total = window_total + jnp.where(
            inside, extended[15 - offset : 15 - offset + row_count], 0.0
        )
    window_mean = window_total / jnp.minimum(length[:, None], window_size[None, :])
    pool_mean = jnp.concatenate(
        [window_mean.reshape(row_count, channels // 4, 4)[..., :3], doc_mean[..., None]], -1
    )
    pool_mean = pool_mean.reshape(row_count, channels)
    pooled = ((pool_mean - values) * pool_gain).astype(jnp.bfloat16)
    terms = jnp.dot(pooled, out_proj, preferred_element_type=jnp.float32)
    projected = lax.psum_scatter(terms.astype(jnp.bfloat16), "tp", scatter_dimension=1, tiled=True)
    hidden_state = residual.astype(jnp.float32) + projected.astype(jnp.float32)
    squares = lax.psum(jnp.sum(hidden_state * hidden_state, axis=1), "tp")
    model_width = residual.shape[1] * lax.axis_size("tp")
    scaling = lax.rsqrt(squares / model_width + 1e-06)
    normed_columns = (hidden_state * scaling[:, None] * norm_gain).astype(jnp.bfloat16)
    normed = lax.all_gather(normed_columns, "tp", axis=1, tiled=True)
    shared_gate_out = jnp.dot(normed, shared_gate, preferred_element_type=jnp.float32)
    shared_up_out = jnp.dot(normed, shared_up, preferred_element_type=jnp.float32)
    shared_hidden = (jax.nn.silu(shared_gate_out) * shared_up_out).astype(jnp.bfloat16)
    shared_terms = jnp.dot(shared_hidden, shared_down, preferred_element_type=jnp.float32)
    group_size = lax.axis_size("tp")
    experts = expert_gate.shape[0] * lax.axis_size("sp")
    top = routes.shape[1]
    capacity = group_size * max(1, 2 * row_count * top // (experts * group_size))
    flat_experts = routes.reshape(-1)
    onehot = (flat_experts[:, None] == jnp.arange(experts, dtype=jnp.int32)[None, :]).astype(
        jnp.int32
    )
    ranks = jnp.sum((jnp.cumsum(onehot, axis=0) - 1) * onehot, axis=1)
    slots = flat_experts * capacity + ranks
    token_index = jnp.arange(row_count * top, dtype=jnp.int32) // top
    slot_token = jnp.full((experts * capacity,), row_count, jnp.int32).at[slots].set(token_index)
    with_blank = jnp.concatenate([normed, jnp.zeros((1, normed.shape[1]), jnp.bfloat16)], 0)
    outgoing = jnp.take(with_blank, slot_token, axis=0).reshape(experts, capacity, normed.shape[1])
    share = capacity // group_size
    mine = lax.dynamic_slice_in_dim(outgoing, lax.axis_index("tp") * share, share, 1)
    arrived = lax.all_to_all(mine, "sp", split_axis=0, concat_axis=0, tiled=True)
    run_arrived = lax.all_gather(arrived, "tp", axis=1, tiled=True)
    expert_parts = expert_terms(run_arrived, expert_gate, expert_up, expert_down)
    routed_sum, shared_sum = (
        lax.psum_scatter(
            expert_parts.astype(jnp.bfloat16), "tp", scatter_dimension=2, tiled=True
        ).astype(jnp.float32),
        lax.psum_scatter(
            shared_terms[None].astype(jnp.bfloat16), "tp", scatter_dimension=2, tiled=True
        ).astype(jnp.float32),
    )
    returned = lax.all_to_all(
        routed_sum.astype(jnp.bfloat16), "sp", split_axis=0, concat_axis=0, tiled=True
    )
    flat_back = returned.reshape(experts * capacity, returned.shape[2])
    picked = (
        jnp.take(flat_back, slots, axis=0).astype(jnp.float32) * route_weights.reshape(-1)[:, None]
    )
    routed = jnp.sum(picked.reshape(row_count, top, flat_back.shape[1]), axis=1)
    shared_out = shared_sum[0].astype(jnp.bfloat16).astype(jnp.float32)
    return (hidden_state + routed + shared_out).astype(jnp.bfloat16)


F32 = jnp.float32
BF16 = jnp.bfloat16


def dot(a, b):
    return jnp.dot(a, b, preferred_element_type=F32)


def silu(v):
    return v * jax.nn.sigmoid(v)


def layer_kernel(
    groups,
    pool_hbm, doc_hbm, routes_hbm, weights_hbm, resid_hbm, gain_hbm, ngain_hbm, oproj_hbm, eg_hbm, eu_hbm, ed_hbm, sg_hbm, su_hbm, sd_hbm,
    out_ref,
    pool_ref, doc_ref, routes_ref, weights_ref, resid_ref, gain_ref, ngain_ref, isem,
    oproj, eg, eu, ed, sg, su, sd, wsem,
    stat_out, stat_in, halo_in, stat_ss, stat_rs, halo_sem,
    s1, p1, q1, z1, r1_ss, r1_rs,
    ss_out, ss_in, ss_ss, ss_rs,
    sel, both, sc_out, sc_in, sc_ss, sc_rs, disp, rows, d_ss, d_rs, ag_ss, ag_rs,
    normed_ref, xs, xs_ss, xs_rs,
    s3, p3, q3, z3, r3_ss, r3_rs,
    hid, s2, p2, q2, z2, r2_ss, r2_rs,
    back, ret, b_ss, b_rs,
    hidden_ref,
):
    n = lax.axis_size("sp")
    tps = lax.axis_size("tp")
    me = lax.axis_index("sp")
    mt = lax.axis_index("tp")
    core = lax.rem(mt, 2)
    yy = mt // 2
    mate = yy * 2 + (1 - core)
    across = (1 - yy) * 2 + core
    R, C = pool_ref.shape
    DT = resid_ref.shape[1]
    D = DT * tps
    cap = disp.shape[1]

    def peer(k):
        return me ^ k

    barrier = pltpu.get_barrier_semaphore()
    for k in range(1, n):
        pl.semaphore_signal(barrier, inc=1, device_id={"sp": peer(k)},
                            device_id_type=pl.DeviceIdType.MESH)
    for j in range(1, tps):
        pl.semaphore_signal(barrier, inc=1, device_id={"tp": lax.rem(mt + j, tps)},
                            device_id_type=pl.DeviceIdType.MESH)

    small = [
        pltpu.make_async_copy(src, dst, isem.at[i])
        for i, (src, dst) in enumerate((
            (doc_hbm, doc_ref), (pool_hbm, pool_ref), (routes_hbm, routes_ref), (gain_hbm, gain_ref),
            (resid_hbm, resid_ref), (ngain_hbm, ngain_ref), (weights_hbm, weights_ref)))
    ]
    loads = [
        pltpu.make_async_copy(src, dst, wsem.at[i])
        for i, (src, dst) in enumerate((
            (oproj_hbm, oproj), (sg_hbm, sg), (su_hbm, su), (sd_hbm, sd),
            (eg_hbm.at[0], eg), (eu_hbm.at[0], eu), (ed_hbm.at[0], ed)))
    ]
    for load in small + loads:
        load.start()
    sends = []

    def send(src, dst, ss, rs, where):
        copy = pltpu.make_async_remote_copy(
            src_ref=src, dst_ref=dst, send_sem=ss, recv_sem=rs,
            device_id=where, device_id_type=pl.DeviceIdType.MESH)
        copy.start()
        sends.append(copy)

    def arrived(ref, ss, rs, where):
        pltpu.make_async_remote_copy(
            src_ref=ref, dst_ref=ref, send_sem=ss, recv_sem=rs,
            device_id=where, device_id_type=pl.DeviceIdType.MESH).wait_recv()

    small[0].wait()
    small[1].wait()
    doc = doc_ref[...].astype(F32)
    first = jnp.min(doc, axis=1, keepdims=True)
    last = jnp.max(doc, axis=1, keepdims=True)
    pool = pool_ref[...]
    tail_mask = jnp.broadcast_to((doc == last).astype(F32), (8, R))
    stat_out[...] = jnp.zeros_like(stat_out)
    stat_out[0:1, :] = dot(tail_mask.astype(BF16), pool)[0:1]
    stat_out[1:2, :] = jnp.broadcast_to(last, (1, C))
    stat_out[2:3, :] = jnp.broadcast_to(jnp.sum(tail_mask[0:1], axis=1, keepdims=True), (1, C))
    stat_out[3:4, 0:R] = pltpu.roll(jnp.broadcast_to(doc, (8, R)), 16, axis=1)[0:1]

    t_pos = lax.broadcasted_iota(jnp.int32, (R, R), 0)
    u_pos = lax.broadcasted_iota(jnp.int32, (R, R), 1)
    gap = t_pos - u_pos
    doc_row = jnp.broadcast_to(doc, (R, R))
    doc_col = doc_row.T

    pl.semaphore_wait(barrier, n - 1 + tps - 1)
    following = jnp.minimum(me + 1, n - 1)

    @pl.when(me < n - 1)
    def _():
        pltpu.make_async_remote_copy(
            src_ref=pool_ref.at[pl.ds(R - 16, 16)], dst_ref=halo_in,
            send_sem=halo_sem.at[0], recv_sem=halo_sem.at[1],
            device_id={"sp": following}, device_id_type=pl.DeviceIdType.MESH).start()

    for k in range(1, n):
        send(stat_out, stat_in.at[k], stat_ss.at[k], stat_rs.at[k], {"sp": peer(k)})

    same = (doc_col == doc_row) & (gap >= 0)
    length = jnp.sum(same.astype(F32), axis=1, keepdims=True)
    windows = (2, 8, 16)
    totals = [dot((same & (gap < w)).astype(F32).astype(BF16), pool) for w in windows]
    totals.append(dot(same.astype(F32).astype(BF16), pool))

    e_iota = lax.broadcasted_iota(jnp.int32, (n, R), 0)
    picked = (e_iota ^ me).astype(F32)
    small[2].wait()
    routes = routes_ref[...].astype(F32)
    r0 = (jnp.broadcast_to(routes[0:1], (n, R)) == picked).astype(F32)
    r1 = (jnp.broadcast_to(routes[1:2], (n, R)) == picked).astype(F32)
    member = r0 + r1
    rank = dot(member.astype(BF16), (gap < 0).astype(F32).astype(BF16))
    slot = lax.broadcasted_iota(jnp.int32, (cap, R), 0).astype(F32)
    for p in range(n):
        here = (jnp.broadcast_to(rank[p:p + 1], (cap, R)) == slot).astype(F32)
        sel[0, p * cap:(p + 1) * cap, :] = (here * r0[p:p + 1]).astype(BF16)
        sel[1, p * cap:(p + 1) * cap, :] = (here * r1[p:p + 1]).astype(BF16)
        both[p * cap:(p + 1) * cap, :] = (here * member[p:p + 1]).astype(BF16)

    @pl.when(me > 0)
    def _():
        arrived(halo_in, halo_sem.at[0], halo_sem.at[1], {"sp": peer(1)})

    for k in range(1, n):
        arrived(stat_in.at[k], stat_ss.at[k], stat_rs.at[k], {"sp": peer(k)})
    carry = jnp.zeros((1, C), F32)
    carry_length = jnp.zeros((1, 1), F32)
    before_doc = jnp.zeros((1, R), F32)
    for k in range(1, n):
        source = jnp.full((1, C), peer(k), jnp.int32)
        use = (stat_in[k, 1:2, :] == jnp.broadcast_to(first, (1, C))) & (source < me)
        carry = carry + jnp.where(use, stat_in[k, 0:1, :], 0.0)
        carry_length = carry_length + jnp.where(use, stat_in[k, 2:3, :], 0.0)[:, 0:1]
        before_doc = before_doc + jnp.where(source[:, 0:R] == me - 1, stat_in[k, 3:4, 0:R], 0.0)
    in_first = (doc_col == first).astype(F32)[:, 0:1]
    length = length + in_first * carry_length
    halo_doc = jnp.broadcast_to(before_doc, (R, R))
    reach = gap + 16
    halo_ok = (halo_doc == doc_col) & (jnp.full((R, R), me, jnp.int32) > 0)
    halo = jnp.where(jnp.full(halo_in.shape, me, jnp.int32) > 0, halo_in[...].astype(F32), 0.0).astype(BF16)
    totals = [
        total + dot((halo_ok & (reach < w)).astype(F32)[:, 0:16].astype(BF16), halo)
        for total, w in zip(totals, windows)
    ] + [totals[3] + in_first * carry]
    lane = lax.rem(lax.broadcasted_iota(jnp.int32, (R, C), 1), 4)
    mean = totals[3] / length
    for i, w in enumerate(windows):
        mean = jnp.where(lane == i, totals[i] / jnp.minimum(length, float(w)), mean)
    small[3].wait()
    pooled = ((mean - pool.astype(F32)) * gain_ref[...]).astype(BF16)

    def scatter_start(s, p, ss, rs):
        for i, y2 in enumerate((1 - yy, yy)):
            send(s.at[y2 * 2 + 1 - core], p.at[i], ss.at[i], rs.at[i], {"tp": mate})

    def scatter_across(s, p, q, z, ss, rs):
        arrived(p.at[0], ss.at[0], rs.at[0], {"tp": mate})
        q[...] = (s[across].astype(F32) + p[0].astype(F32)).astype(BF16)
        send(q, z, ss.at[2], rs.at[2], {"tp": across})

    def scatter_end(s, p, z, ss, rs):
        arrived(p.at[1], ss.at[1], rs.at[1], {"tp": mate})
        own = s[mt].astype(F32) + p[1].astype(F32)
        arrived(z, ss.at[2], rs.at[2], {"tp": across})
        return own + z[...].astype(F32)

    loads[0].wait()
    for j in range(tps):
        s1[j] = dot(pooled, oproj[:, j * DT:(j + 1) * DT]).astype(BF16)
    scatter_start(s1, p1, r1_ss, r1_rs)
    scatter_across(s1, p1, q1, z1, r1_ss, r1_rs)
    projected = scatter_end(s1, p1, z1, r1_ss, r1_rs)
    for load in small[4:]:
        load.wait()
    hidden = resid_ref[...].astype(F32) + projected
    hidden_ref[...] = hidden
    squares = jnp.sum(hidden * hidden, axis=1, keepdims=True)
    sq_row = jnp.broadcast_to(squares, (R, R)).T
    ss_out[...] = sq_row[0:8]
    for j in range(1, tps):
        send(ss_out, ss_in.at[j], ss_ss.at[j], ss_rs.at[j], {"tp": lax.rem(mt + j, tps)})
    normed = (hidden * ngain_ref[...]).astype(BF16)
    normed_ref[...] = normed

    send(normed_ref, xs.at[mt], xs_ss.at[0], xs_rs.at[0], {"tp": across})
    send(normed_ref, xs.at[mt], xs_ss.at[1], xs_rs.at[1], {"tp": mate})
    for ps in (list(range(1, n // 2)), list(range(n // 2, n))):
        span = slice(ps[0] * cap, (ps[-1] + 1) * cap)
        disp[ps[0]:ps[-1] + 1] = dot(both[span, :], normed).astype(BF16).reshape(len(ps), cap, DT)
        for p in ps:
            send(disp.at[p], rows.at[p, mt], d_ss.at[p], d_rs.at[p], {"sp": peer(p)})
    xs[mt] = normed

    all_sq = sq_row[0:8]
    for j in range(1, tps):
        arrived(ss_in.at[j], ss_ss.at[j], ss_rs.at[j], {"tp": mt})
        all_sq = all_sq + ss_in[j]
    scale_row = lax.rsqrt(all_sq / D + 1e-06)
    high = scale_row.astype(BF16)
    rest = scale_row - high.astype(F32)
    middle = rest.astype(BF16)
    low = (rest - middle.astype(F32)).astype(BF16)
    turned = (((1,), (1,)), ((), ()))
    slot_scale = sum(
        lax.dot_general(part, both[...], turned, preferred_element_type=F32) for part in (high, middle, low))
    for p in range(n):
        sc_out[p, :, 0:cap] = slot_scale[:, p * cap:(p + 1) * cap]
        if p:
            send(sc_out.at[p], sc_in.at[p], sc_ss.at[p], sc_rs.at[p], {"sp": peer(p)})
    scale = jnp.broadcast_to(scale_row[0:1], (R, R)).T[:, 0:1]

    def own_here(p):
        arrived(rows.at[p, mt], d_ss.at[p], d_rs.at[p], {"sp": peer(p)})

    def forward_own(*ps):
        for p in ps:
            own_here(p)
            send(rows.at[p, mt], rows.at[p, mt], ag_ss.at[p, 0], ag_rs.at[p, 0], {"tp": across})
            send(rows.at[p, mt], rows.at[p, mt], ag_ss.at[p, 1], ag_rs.at[p, 1], {"tp": mate})

    def forward_own2(*ps):
        for p in ps:
            send(rows.at[p, mt], rows.at[p, mt], ag_ss.at[p, 0], ag_rs.at[p, 0], {"tp": across})
            send(rows.at[p, mt], rows.at[p, mt], ag_ss.at[p, 1], ag_rs.at[p, 1], {"tp": mate})

    def forward_across(*ps):
        for p in ps:
            arrived(rows.at[p, across], ag_ss.at[p, 0], ag_rs.at[p, 0], {"tp": across})
            send(rows.at[p, across], rows.at[p, across], ag_ss.at[p, 2], ag_rs.at[p, 2], {"tp": mate})

    def all_here(*ps):
        for p in ps:
            if p:
                arrived(rows.at[p, mate], ag_ss.at[p, 1], ag_rs.at[p, 1], {"tp": mate})
                arrived(rows.at[p, (1 - yy) * 2 + 1 - core], ag_ss.at[p, 2], ag_rs.at[p, 2], {"tp": mate})
                arrived(sc_in.at[p], sc_ss.at[p], sc_rs.at[p], {"sp": peer(p)})

    def xs_across():
        arrived(xs.at[across], xs_ss.at[0], xs_rs.at[0], {"tp": across})
        send(xs.at[across], xs.at[across], xs_ss.at[2], xs_rs.at[2], {"tp": mate})

    def xs_rest():
        arrived(xs.at[mate], xs_ss.at[1], xs_rs.at[1], {"tp": mate})
        arrived(xs.at[(1 - yy) * 2 + 1 - core], xs_ss.at[2], xs_rs.at[2], {"tp": mate})
        for j in range(tps):
            rows[0, j] = dot(both[0:cap, :], xs[j]).astype(BF16)

    def weights_here():
        for load in loads[4:]:
            load.wait()

    def shared():
        for load in loads[1:4]:
            load.wait()
        g = sum(dot(xs[j], sg[j * DT:(j + 1) * DT, :]) for j in range(tps)) * scale
        u = sum(dot(xs[j], su[j * DT:(j + 1) * DT, :]) for j in range(tps)) * scale
        hs = (silu(g) * u).astype(BF16)
        for j in range(tps):
            s3[j] = dot(hs, sd[:, j * DT:(j + 1) * DT]).astype(BF16)
        scatter_start(s3, p3, r3_ss, r3_rs)

    def shared_across():
        scatter_across(s3, p3, q3, z3, r3_ss, r3_rs)

    def shared_end():
        hidden_ref[...] = hidden_ref[...] + scatter_end(s3, p3, z3, r3_ss, r3_rs).astype(BF16).astype(F32)

    FF = eg.shape[1]
    tile = 256 if FF % 256 == 0 else FF
    tiles = FF // tile

    def expert_up(gi, start=0, stop=tiles):
        ps = groups[gi]
        m = len(ps) * cap
        factors = []
        for p in ps:
            line = (sc_in if p else sc_out)[p, 0:1, :]
            factors.append(jnp.broadcast_to(line, (128, 128)).T[0:cap, 0:1])
        factor = jnp.concatenate(factors, 0)
        span = pl.ds(ps[0] * cap, m)

        def up(i, _):
            cols = pl.ds(pl.multiple_of(i * tile, tile), tile)
            a = jnp.zeros((m, tile), F32)
            b = jnp.zeros((m, tile), F32)
            for j in range(tps):
                x = rows[ps[0]:ps[0] + len(ps), j].reshape(m, DT)
                a = a + dot(x, eg[j * DT:(j + 1) * DT, cols])
                b = b + dot(x, eu[j * DT:(j + 1) * DT, cols])
            hid[span, cols] = (silu(a * factor) * (b * factor)).astype(BF16)
            return 0

        lax.fori_loop(start, stop, up, 0)

    def expert_down(gi, half):
        span = pl.ds(groups[gi][0] * cap, len(groups[gi]) * cap)
        s, p, _, _, ss, rs = scatter_refs(gi)

        def down(j):
            s[j] = dot(hid[span, :], ed[:, pl.ds(pl.multiple_of(j * DT, DT), DT)]).astype(BF16)

        for i, y2 in enumerate((1 - yy, yy)):
            if i in half:
                down(y2 * 2 + 1 - core)
                send(s.at[y2 * 2 + 1 - core], p.at[i], ss.at[i], rs.at[i], {"tp": mate})
                down(y2 * 2 + core)

    def scatter_refs(gi):
        span = pl.ds(groups[gi][0] * cap, len(groups[gi]) * cap)
        return (s2.at[:, span], p2.at[:, span], q2.at[span], z2.at[span], r2_ss.at[gi], r2_rs.at[gi])

    def across2(gi):
        scatter_across(*scatter_refs(gi))

    def give_back(gi):
        s, p, q, z, ss, rs = scatter_refs(gi)
        total = scatter_end(s, p, z, ss, rs).astype(BF16)
        for i, p in enumerate(groups[gi]):
            piece = total[i * cap:(i + 1) * cap]
            if p == 0:
                ret[0:cap, :] = piece
            else:
                back[p] = piece
                send(back.at[p], ret.at[pl.ds(p * cap, cap)], b_ss.at[p], b_rs.at[p], {"sp": peer(p)})

    def collect(gi):
        span = pl.ds(groups[gi][0] * cap, len(groups[gi]) * cap)
        for p in groups[gi]:
            if p:
                arrived(ret.at[pl.ds(p * cap, cap)], b_ss.at[p], b_rs.at[p], {"sp": peer(p)})
        total = hidden_ref[...]
        for k in range(2):
            weight = jnp.broadcast_to(weights_ref[k:k + 1, :], (R, R)).T[:, 0:1]
            chosen = lax.dot_general(
                sel[k, span], ret[span], (((0,), (0,)), ((), ())), preferred_element_type=F32)
            total = total + weight * chosen
        hidden_ref[...] = total

    forward_own(1)
    xs_across()
    forward_own(2)
    forward_own(4)
    forward_across(1)
    xs_rest()
    forward_own(5)
    weights_here()
    all_here(0, 1)
    expert_up(0, 0, 2)
    forward_own(3)
    forward_across(2, 4)
    expert_up(0, 2, 4)
    forward_across(5)
    forward_own(6)
    expert_down(0, (0,))
    forward_across(3)
    expert_down(0, (1,))
    forward_own(7)
    all_here(4, 5)
    expert_up(2, 0, 2)
    forward_across(6)
    across2(0)
    expert_up(2, 2, 4)
    expert_down(2, (0, 1))
    forward_across(7)
    shared()
    across2(2)
    all_here(6, 7)
    expert_up(3)
    give_back(0)
    expert_down(3, (0, 1))
    all_here(2, 3)
    expert_up(1, 0, 2)
    across2(3)
    give_back(2)
    expert_up(1, 2, 4)
    expert_down(1, (0, 1))
    collect(0)
    give_back(3)
    across2(1)
    shared_across()
    collect(2)
    give_back(1)
    shared_end()
    collect(3)
    collect(1)
    out_ref[...] = hidden_ref[...].astype(BF16)
    for copy in sends:
        copy.wait_send()

    @pl.when(me < n - 1)
    def _():
        pltpu.make_async_remote_copy(
            src_ref=pool_ref.at[pl.ds(R - 16, 16)], dst_ref=halo_in,
            send_sem=halo_sem.at[0], recv_sem=halo_sem.at[1],
            device_id={"sp": following}, device_id_type=pl.DeviceIdType.MESH).wait_send()


def body(
    pool_input, doc_ids, residual, pool_gain, out_proj, norm_gain, routes, route_weights,
    expert_gate, expert_up, expert_down, shared_gate, shared_up, shared_down,
):
    n, tps = lax.axis_size("sp"), lax.axis_size("tp")
    R, C = pool_input.shape
    DT = residual.shape[1]
    FF, FS, D = expert_gate.shape[2], shared_gate.shape[1], expert_gate.shape[1]
    experts = expert_gate.shape[0] * n
    top = routes.shape[1]
    cap = tps * max(1, 2 * R * top // (experts * tps))
    groups = [[0, 1], [2, 3], [4, 5], [6, 7]]
    V, DMA = pltpu.VMEM, pltpu.SemaphoreType.DMA
    scratch = [
        V((R, C), BF16), V((1, R), jnp.int32), V((top, R), jnp.int32), V((top, R), F32),
        V((R, DT), BF16), V((1, C), F32), V((1, DT), F32), DMA((7,)),
        V((C, D), BF16), V((D, FF), BF16), V((D, FF), BF16), V((FF, D), BF16),
        V((D, FS), BF16), V((D, FS), BF16), V((FS, D), BF16), DMA((7,)),
        V((8, C), F32), V((n, 8, C), F32), V((16, C), BF16), DMA((n,)), DMA((n,)), DMA((2,)),
        V((tps, R, DT), BF16), V((2, R, DT), BF16), V((R, DT), BF16), V((R, DT), BF16), DMA((3,)), DMA((3,)),
        V((8, R), F32), V((tps, 8, R), F32), DMA((tps,)), DMA((tps,)),
        V((2, n * cap, R), BF16), V((n * cap, R), BF16), V((n, 8, 128), F32), V((n, 8, 128), F32), DMA((n,)), DMA((n,)),
        V((n, cap, DT), BF16), V((n, tps, cap, DT), BF16),
        DMA((n,)), DMA((n,)), DMA((n, 3)), DMA((n, 3)),
        V((R, DT), BF16), V((tps, R, DT), BF16), DMA((3,)), DMA((3,)),
        V((tps, R, DT), BF16), V((2, R, DT), BF16), V((R, DT), BF16), V((R, DT), BF16), DMA((3,)), DMA((3,)),
        V((n * cap, FF), BF16), V((tps, n * cap, DT), BF16), V((2, n * cap, DT), BF16),
        V((n * cap, DT), BF16), V((n * cap, DT), BF16), DMA((len(groups), 3)), DMA((len(groups), 3)),
        V((n, cap, DT), BF16), V((n * cap, DT), BF16), DMA((n,)), DMA((n,)),
        V((R, DT), F32),
    ]
    vm = pl.BlockSpec(memory_space=pltpu.VMEM)
    hb = pl.BlockSpec(memory_space=pltpu.HBM)
    return pl.pallas_call(
        functools.partial(layer_kernel, groups),
        out_shape=jax.ShapeDtypeStruct((R, DT), BF16),
        in_specs=[hb] * 14,
        out_specs=vm,
        scratch_shapes=scratch,
        compiler_params=pltpu.CompilerParams(
            collective_id=0, has_side_effects=True, vmem_limit_bytes=60 * 2**20),
    )(pool_input, doc_ids.reshape(1, R), routes.T, route_weights.T, residual, pool_gain.reshape(1, C), norm_gain.reshape(1, DT),
      out_proj, expert_gate, expert_up, expert_down, shared_gate, shared_up, shared_down)


def one_kernel_fits(mesh):
    return mesh.shape["tp"] == 4 and mesh.shape["sp"] == 8


def solution(mesh):
    placed = (
        P("sp", "tp"),
        P("sp"),
        P("sp", "tp"),
        P("tp"),
        P("tp", None),
        P("tp"),
        P("sp", None),
        P("sp", None),
        P("sp", None, "tp"),
        P("sp", None, "tp"),
        P("sp", "tp", None),
        P(None, "tp"),
        P(None, "tp"),
        P("tp", None),
    )
    return jax.shard_map(
        body if one_kernel_fits(mesh) else plain_body, mesh=mesh, in_specs=placed, out_specs=P("sp", "tp"), check_vma=False)
```

```python
import jax
import functools
import jax.numpy as jnp
from jax import lax
from jax.experimental import pallas as pl
from jax.experimental.pallas import tpu as pltpu
from jax.sharding import PartitionSpec as P


def carried_in(value, axis, join, neutral):
    count, mine = (lax.axis_size(axis), lax.axis_index(axis))
    pieces = jax.tree.map(lambda part: lax.all_gather(part, axis), value)
    subtotal = jax.tree.map(
        lambda part, zero: jnp.full_like(part, 0) + jnp.asarray(zero, part.dtype), value, neutral
    )

    def hop(position, subtotal):
        longer = join(subtotal, jax.tree.map(lambda part: part[position], pieces))
        return jax.tree.map(lambda new, old: jnp.where(position < mine, new, old), longer, subtotal)

    return lax.fori_loop(0, count - 1, hop, subtotal)


def from_behind(value, axis, by):
    size = lax.axis_size(axis)
    pairs = [(i, i + by) for i in range(size) if 0 <= i + by < size]
    return lax.ppermute(value, axis, pairs)


def join_documents(earlier, later):
    earlier_sum, earlier_length, earlier_first, earlier_last, earlier_inner = earlier
    later_sum, later_length, later_first, later_last, later_inner = later
    boundary = later_first != earlier_last
    restart = (later_inner > 0) | boundary
    merged = (
        jnp.where(restart, later_sum, earlier_sum + later_sum),
        jnp.where(restart, later_length, earlier_length + later_length),
        earlier_first,
        later_last,
        jnp.maximum(jnp.maximum(earlier_inner, later_inner), boundary.astype(jnp.float32)),
    )
    earlier_empty = earlier_first < 0
    later_empty = later_first < 0
    return tuple(
        (
            jnp.where(earlier_empty, second, jnp.where(later_empty, first_value, joined))
            for first_value, second, joined in zip(earlier, later, merged)
        )
    )


def expert_terms(arrived, gate_weight, up_weight, down_weight):
    local_experts = gate_weight.shape[0]
    sources = arrived.shape[0] // local_experts
    grouped = arrived.reshape(sources, local_experts, arrived.shape[1], arrived.shape[2])
    gate = jnp.einsum("secd,edf->secf", grouped, gate_weight, preferred_element_type=jnp.float32)
    upper = jnp.einsum("secd,edf->secf", grouped, up_weight, preferred_element_type=jnp.float32)
    hidden = (jax.nn.silu(gate) * upper).astype(jnp.bfloat16)
    output = jnp.einsum("secf,efd->secd", hidden, down_weight, preferred_element_type=jnp.float32)
    return output.reshape(arrived.shape[0], arrived.shape[1], down_weight.shape[2])


def plain_body(
    pool_input,
    doc_ids,
    residual,
    pool_gain,
    out_proj,
    norm_gain,
    routes,
    route_weights,
    expert_gate,
    expert_up,
    expert_down,
    shared_gate,
    shared_up,
    shared_down,
):
    row_count, channels = pool_input.shape
    values = pool_input.astype(jnp.float32)
    positions = jnp.arange(row_count, dtype=jnp.int32)
    inner_begin = jnp.concatenate([jnp.zeros((1,), bool), doc_ids[1:] != doc_ids[:-1]])
    running = jnp.cumsum(values[:, 3::4], axis=0)
    shifted = jnp.concatenate([jnp.zeros((1, running.shape[1]), jnp.float32), running], 0)
    inner_last = jnp.max(jnp.where(inner_begin, positions, 0))
    own_terms = (
        running[-1] - shifted[inner_last],
        (row_count - inner_last).astype(jnp.float32),
        doc_ids[0].astype(jnp.float32),
        doc_ids[-1].astype(jnp.float32),
        jnp.any(inner_begin).astype(jnp.float32),
    )
    identity = (
        jnp.zeros((running.shape[1],), jnp.float32),
        jnp.zeros((), jnp.float32),
        jnp.full((), -1.0, jnp.float32),
        jnp.full((), -1.0, jnp.float32),
        jnp.zeros((), jnp.float32),
    )
    before = carried_in(own_terms, "sp", join_documents, identity)
    fresh = (before[2] < 0) | (doc_ids[0].astype(jnp.float32) != before[3])
    begins = jnp.concatenate([fresh[None], inner_begin[1:]])
    doc_start = lax.cummax(jnp.where(begins, positions, -1), axis=0)
    found = doc_start >= 0
    carry_sum = jnp.where(fresh, 0.0, before[0])
    carry_length = jnp.where(fresh, 0.0, before[1])
    length = jnp.where(
        found,
        (positions - doc_start + 1).astype(jnp.float32),
        carry_length + (positions + 1).astype(jnp.float32),
    )
    start_rows = jnp.take(shifted, jnp.maximum(doc_start, 0), axis=0)
    doc_sum = jnp.where(found[:, None], running - start_rows, carry_sum[None, :] + running)
    doc_mean = doc_sum / length[:, None]
    rim = from_behind(pool_input[row_count - 15 :], "sp", 1)
    extended = jnp.concatenate([rim, pool_input], 0).astype(jnp.float32)
    scale_index = jnp.arange(channels, dtype=jnp.int32) % 4
    window_size = jnp.where(scale_index == 0, 2.0, jnp.where(scale_index == 1, 8.0, 16.0))
    window_total = jnp.zeros((row_count, channels), jnp.float32)
    for offset in range(16):
        inside = (offset < length[:, None]) & (offset < window_size[None, :])
        window_total = window_total + jnp.where(
            inside, extended[15 - offset : 15 - offset + row_count], 0.0
        )
    window_mean = window_total / jnp.minimum(length[:, None], window_size[None, :])
    pool_mean = jnp.concatenate(
        [window_mean.reshape(row_count, channels // 4, 4)[..., :3], doc_mean[..., None]], -1
    )
    pool_mean = pool_mean.reshape(row_count, channels)
    pooled = ((pool_mean - values) * pool_gain).astype(jnp.bfloat16)
    terms = jnp.dot(pooled, out_proj, preferred_element_type=jnp.float32)
    projected = lax.psum_scatter(terms.astype(jnp.bfloat16), "tp", scatter_dimension=1, tiled=True)
    hidden_state = residual.astype(jnp.float32) + projected.astype(jnp.float32)
    squares = lax.psum(jnp.sum(hidden_state * hidden_state, axis=1), "tp")
    model_width = residual.shape[1] * lax.axis_size("tp")
    scaling = lax.rsqrt(squares / model_width + 1e-06)
    normed_columns = (hidden_state * scaling[:, None] * norm_gain).astype(jnp.bfloat16)
    normed = lax.all_gather(normed_columns, "tp", axis=1, tiled=True)
    shared_gate_out = jnp.dot(normed, shared_gate, preferred_element_type=jnp.float32)
    shared_up_out = jnp.dot(normed, shared_up, preferred_element_type=jnp.float32)
    shared_hidden = (jax.nn.silu(shared_gate_out) * shared_up_out).astype(jnp.bfloat16)
    shared_terms = jnp.dot(shared_hidden, shared_down, preferred_element_type=jnp.float32)
    group_size = lax.axis_size("tp")
    experts = expert_gate.shape[0] * lax.axis_size("sp")
    top = routes.shape[1]
    capacity = group_size * max(1, 2 * row_count * top // (experts * group_size))
    flat_experts = routes.reshape(-1)
    onehot = (flat_experts[:, None] == jnp.arange(experts, dtype=jnp.int32)[None, :]).astype(
        jnp.int32
    )
    ranks = jnp.sum((jnp.cumsum(onehot, axis=0) - 1) * onehot, axis=1)
    slots = flat_experts * capacity + ranks
    token_index = jnp.arange(row_count * top, dtype=jnp.int32) // top
    slot_token = jnp.full((experts * capacity,), row_count, jnp.int32).at[slots].set(token_index)
    with_blank = jnp.concatenate([normed, jnp.zeros((1, normed.shape[1]), jnp.bfloat16)], 0)
    outgoing = jnp.take(with_blank, slot_token, axis=0).reshape(experts, capacity, normed.shape[1])
    share = capacity // group_size
    mine = lax.dynamic_slice_in_dim(outgoing, lax.axis_index("tp") * share, share, 1)
    arrived = lax.all_to_all(mine, "sp", split_axis=0, concat_axis=0, tiled=True)
    run_arrived = lax.all_gather(arrived, "tp", axis=1, tiled=True)
    expert_parts = expert_terms(run_arrived, expert_gate, expert_up, expert_down)
    routed_sum, shared_sum = (
        lax.psum_scatter(
            expert_parts.astype(jnp.bfloat16), "tp", scatter_dimension=2, tiled=True
        ).astype(jnp.float32),
        lax.psum_scatter(
            shared_terms[None].astype(jnp.bfloat16), "tp", scatter_dimension=2, tiled=True
        ).astype(jnp.float32),
    )
    returned = lax.all_to_all(
        routed_sum.astype(jnp.bfloat16), "sp", split_axis=0, concat_axis=0, tiled=True
    )
    flat_back = returned.reshape(experts * capacity, returned.shape[2])
    picked = (
        jnp.take(flat_back, slots, axis=0).astype(jnp.float32) * route_weights.reshape(-1)[:, None]
    )
    routed = jnp.sum(picked.reshape(row_count, top, flat_back.shape[1]), axis=1)
    shared_out = shared_sum[0].astype(jnp.bfloat16).astype(jnp.float32)
    return (hidden_state + routed + shared_out).astype(jnp.bfloat16)


F32 = jnp.float32
BF16 = jnp.bfloat16


def dot(a, b):
    return jnp.dot(a, b, preferred_element_type=F32)


def silu(v):
    return v * jax.nn.sigmoid(v)


def layer_kernel(
    groups,
    pool_hbm, doc_hbm, routes_hbm, weights_hbm, resid_hbm, gain_hbm, ngain_hbm, oproj_hbm, eg_hbm, eu_hbm, ed_hbm, sg_hbm, su_hbm, sd_hbm,
    out_ref,
    pool_ref, doc_ref, routes_ref, weights_ref, resid_ref, gain_ref, ngain_ref, isem,
    oproj, eg, eu, ed, sg, su, sd, wsem,
    stat_out, stat_in, halo_in, stat_ss, stat_rs, halo_sem,
    s1, p1, q1, z1, r1_ss, r1_rs,
    ss_out, ss_in, ss_ss, ss_rs,
    sel, both, sc_out, sc_in, sc_ss, sc_rs, disp, rows, d_ss, d_rs, ag_ss, ag_rs,
    normed_ref, xs, xs_ss, xs_rs,
    s3, p3, q3, z3, r3_ss, r3_rs,
    hid, s2, p2, q2, z2, r2_ss, r2_rs, q_ss, q_rs,
    back, ret, b_ss, b_rs,
    hidden_ref,
):
    n = lax.axis_size("sp")
    tps = lax.axis_size("tp")
    me = lax.axis_index("sp")
    mt = lax.axis_index("tp")
    core = lax.rem(mt, 2)
    yy = mt // 2
    mate = yy * 2 + (1 - core)
    across = (1 - yy) * 2 + core
    R, C = pool_ref.shape
    DT = resid_ref.shape[1]
    D = DT * tps
    cap = disp.shape[1]

    def key(p):
        return (p & 1) | ((p & 2) << 1) | ((p & 4) >> 1)

    def peer(p):
        return me ^ key(p)

    barrier = pltpu.get_barrier_semaphore()
    for k in range(1, n):
        pl.semaphore_signal(barrier, inc=1, device_id={"sp": peer(k)},
                            device_id_type=pl.DeviceIdType.MESH)
    for j in range(1, tps):
        pl.semaphore_signal(barrier, inc=1, device_id={"tp": lax.rem(mt + j, tps)},
                            device_id_type=pl.DeviceIdType.MESH)

    small = [
        pltpu.make_async_copy(src, dst, isem.at[i])
        for i, (src, dst) in enumerate((
            (doc_hbm, doc_ref), (pool_hbm, pool_ref), (routes_hbm, routes_ref), (gain_hbm, gain_ref),
            (resid_hbm, resid_ref), (ngain_hbm, ngain_ref), (weights_hbm, weights_ref)))
    ]
    loads = [
        pltpu.make_async_copy(src, dst, wsem.at[i])
        for i, (src, dst) in enumerate((
            (oproj_hbm, oproj), (sg_hbm, sg), (su_hbm, su), (sd_hbm, sd),
            (eg_hbm.at[0], eg), (eu_hbm.at[0], eu), (ed_hbm.at[0], ed)))
    ]
    for load in small + loads:
        load.start()
    sends = []

    def send(src, dst, ss, rs, where):
        copy = pltpu.make_async_remote_copy(
            src_ref=src, dst_ref=dst, send_sem=ss, recv_sem=rs,
            device_id=where, device_id_type=pl.DeviceIdType.MESH)
        copy.start()
        sends.append(copy)

    def arrived(ref, ss, rs, where):
        pltpu.make_async_remote_copy(
            src_ref=ref, dst_ref=ref, send_sem=ss, recv_sem=rs,
            device_id=where, device_id_type=pl.DeviceIdType.MESH).wait_recv()

    small[0].wait()
    small[1].wait()
    doc = doc_ref[...].astype(F32)
    first = jnp.min(doc, axis=1, keepdims=True)
    last = jnp.max(doc, axis=1, keepdims=True)
    pool = pool_ref[...]
    tail_mask = jnp.broadcast_to((doc == last).astype(F32), (8, R))
    stat_out[:, 0:C] = dot(tail_mask.astype(BF16), pool)[0:1]
    stat_out[:, C:C + 128] = jnp.broadcast_to(last, (1, 128))
    stat_out[:, C + 128:C + 256] = jnp.broadcast_to(jnp.sum(tail_mask[0:1], axis=1, keepdims=True), (1, 128))

    t_pos = lax.broadcasted_iota(jnp.int32, (R, R), 0)
    u_pos = lax.broadcasted_iota(jnp.int32, (R, R), 1)
    gap = t_pos - u_pos
    doc_row = jnp.broadcast_to(doc, (R, R))
    doc_col = doc_row.T

    pl.semaphore_wait(barrier, n - 1 + tps - 1)
    following = jnp.minimum(me + 1, n - 1)

    @pl.when(me < n - 1)
    def _():
        pltpu.make_async_remote_copy(
            src_ref=pool_ref.at[pl.ds(R - 16, 16)], dst_ref=halo_in,
            send_sem=halo_sem.at[0], recv_sem=halo_sem.at[1],
            device_id={"sp": following}, device_id_type=pl.DeviceIdType.MESH).start()

    for k in range(1, n):
        send(stat_out, stat_in.at[k], stat_ss.at[k], stat_rs.at[k], {"sp": peer(k)})

    same = (doc_col == doc_row) & (gap >= 0)
    length = jnp.sum(same.astype(F32), axis=1, keepdims=True)
    windows = (2, 8, 16)
    totals = [dot((same & (gap < w)).astype(F32).astype(BF16), pool) for w in windows]
    totals.append(dot(same.astype(F32).astype(BF16), pool))

    e_iota = lax.broadcasted_iota(jnp.int32, (n, R), 0)
    picked = (key(e_iota) ^ me).astype(F32)
    small[2].wait()
    routes = routes_ref[...].astype(F32)
    r0 = (jnp.broadcast_to(routes[0:1], (n, R)) == picked).astype(F32)
    r1 = (jnp.broadcast_to(routes[1:2], (n, R)) == picked).astype(F32)
    member = r0 + r1
    rank = dot(member.astype(BF16), (gap < 0).astype(F32).astype(BF16))
    slot = lax.broadcasted_iota(jnp.int32, (cap, R), 0).astype(F32)
    for p in range(n):
        here = (jnp.broadcast_to(rank[p:p + 1], (cap, R)) == slot).astype(F32)
        sel[0, p * cap:(p + 1) * cap, :] = (here * r0[p:p + 1]).astype(BF16)
        sel[1, p * cap:(p + 1) * cap, :] = (here * r1[p:p + 1]).astype(BF16)
        both[p * cap:(p + 1) * cap, :] = (here * member[p:p + 1]).astype(BF16)

    @pl.when(me > 0)
    def _():
        arrived(halo_in, halo_sem.at[0], halo_sem.at[1], {"sp": peer(1)})

    for k in range(1, n):
        arrived(stat_in.at[k], stat_ss.at[k], stat_rs.at[k], {"sp": peer(k)})
    carry = jnp.zeros((1, C), F32)
    carry_length = jnp.zeros((1, 1), F32)
    before = jnp.zeros((1, R), F32)
    for k in range(1, n):
        source = jnp.full((1, 128), peer(k), jnp.int32)
        use = (stat_in[k, :, C:C + 128] == jnp.broadcast_to(first, (1, 128))) & (source < me)
        tail = jnp.where(use, stat_in[k, :, C + 128:C + 256], 0.0)
        keep = jnp.concatenate([use.astype(F32)] * (C // 128), axis=1)
        carry = carry + keep * stat_in[k, :, 0:C]
        carry_length = carry_length + tail[:, 0:1]
        before = before + jnp.where(source == me - 1, tail, 0.0)
    in_first = (doc_col == first).astype(F32)[:, 0:1]
    length = length + in_first * carry_length
    reach = gap + 16
    halo_ok = (doc_col == first) & (u_pos.astype(F32) >= 16.0 - jnp.broadcast_to(before, (R, R)))
    halo = jnp.where(jnp.full(halo_in.shape, me, jnp.int32) > 0, halo_in[...].astype(F32), 0.0).astype(BF16)
    totals = [
        total + dot((halo_ok & (reach < w)).astype(F32)[:, 0:16].astype(BF16), halo)
        for total, w in zip(totals, windows)
    ] + [totals[3] + in_first * carry]
    lane = lax.rem(lax.broadcasted_iota(jnp.int32, (R, C), 1), 4)
    mean = totals[3] / length
    for i, w in enumerate(windows):
        mean = jnp.where(lane == i, totals[i] / jnp.minimum(length, float(w)), mean)
    small[3].wait()
    pooled = ((mean - pool.astype(F32)) * gain_ref[...]).astype(BF16)

    def scatter_start(s, p, ss, rs):
        for i, y2 in enumerate((1 - yy, yy)):
            send(s.at[y2 * 2 + 1 - core], p.at[i], ss.at[i], rs.at[i], {"tp": mate})

    def scatter_across(s, p, q, z, ss, rs):
        arrived(p.at[0], ss.at[0], rs.at[0], {"tp": mate})
        q[...] = (s[across].astype(F32) + p[0].astype(F32)).astype(BF16)
        send(q, z, ss.at[2], rs.at[2], {"tp": across})

    def scatter_end(s, p, z, ss, rs):
        arrived(p.at[1], ss.at[1], rs.at[1], {"tp": mate})
        own = s[mt].astype(F32) + p[1].astype(F32)
        arrived(z, ss.at[2], rs.at[2], {"tp": across})
        return own + z[...].astype(F32)

    loads[0].wait()
    for j in range(tps):
        s1[j] = dot(pooled, oproj[:, j * DT:(j + 1) * DT]).astype(BF16)
    scatter_start(s1, p1, r1_ss, r1_rs)
    scatter_across(s1, p1, q1, z1, r1_ss, r1_rs)
    projected = scatter_end(s1, p1, z1, r1_ss, r1_rs)
    for load in small[4:]:
        load.wait()
    hidden = resid_ref[...].astype(F32) + projected
    hidden_ref[...] = hidden
    squares = jnp.sum(hidden * hidden, axis=1, keepdims=True)
    sq_row = jnp.broadcast_to(squares, (R, R)).T
    ss_out[...] = sq_row[0:8]
    for j in range(1, tps):
        send(ss_out, ss_in.at[j], ss_ss.at[j], ss_rs.at[j], {"tp": lax.rem(mt + j, tps)})
    normed = (hidden * ngain_ref[...]).astype(BF16)
    normed_ref[...] = normed

    send(normed_ref, xs.at[mt], xs_ss.at[0], xs_rs.at[0], {"tp": across})
    send(normed_ref, xs.at[mt], xs_ss.at[1], xs_rs.at[1], {"tp": mate})
    disp[1:n] = dot(both[cap:, :], normed).astype(BF16).reshape(n - 1, cap, DT)

    def dispatch(*ps):
        for p in ps:
            send(disp.at[p], rows.at[p, mt], d_ss.at[p], d_rs.at[p], {"sp": peer(p)})

    dispatch(1, 4, 5, 2, 3)
    xs[mt] = normed

    all_sq = sq_row[0:8]
    for j in range(1, tps):
        arrived(ss_in.at[j], ss_ss.at[j], ss_rs.at[j], {"tp": mt})
        all_sq = all_sq + ss_in[j]
    scale_row = lax.rsqrt(all_sq / D + 1e-06)
    high = scale_row.astype(BF16)
    rest = scale_row - high.astype(F32)
    middle = rest.astype(BF16)
    low = (rest - middle.astype(F32)).astype(BF16)
    turned = (((1,), (1,)), ((), ()))
    slot_scale = sum(
        lax.dot_general(part, both[...], turned, preferred_element_type=F32) for part in (high, middle, low))
    for p in range(n):
        sc_out[p, :, 0:cap] = slot_scale[0:1, p * cap:(p + 1) * cap]
    for p in (6, 7, 2, 3, 4, 5, 1):
        send(sc_out.at[p], sc_in.at[p], sc_ss.at[p], sc_rs.at[p], {"sp": peer(p)})
    dispatch(6, 7)
    scale = jnp.broadcast_to(scale_row[0:1], (R, R)).T[:, 0:1]

    def own_here(p):
        arrived(rows.at[p, mt], d_ss.at[p], d_rs.at[p], {"sp": peer(p)})

    def forward_own(*ps):
        for p in ps:
            own_here(p)
            send(rows.at[p, mt], rows.at[p, mt], ag_ss.at[p, 0], ag_rs.at[p, 0], {"tp": across})
            send(rows.at[p, mt], rows.at[p, mt], ag_ss.at[p, 1], ag_rs.at[p, 1], {"tp": mate})

    def forward_own2(*ps):
        for p in ps:
            send(rows.at[p, mt], rows.at[p, mt], ag_ss.at[p, 0], ag_rs.at[p, 0], {"tp": across})
            send(rows.at[p, mt], rows.at[p, mt], ag_ss.at[p, 1], ag_rs.at[p, 1], {"tp": mate})

    def forward_across(*ps):
        for p in ps:
            arrived(rows.at[p, across], ag_ss.at[p, 0], ag_rs.at[p, 0], {"tp": across})
            send(rows.at[p, across], rows.at[p, across], ag_ss.at[p, 2], ag_rs.at[p, 2], {"tp": mate})

    def all_here(*ps):
        for p in ps:
            if p:
                arrived(rows.at[p, mate], ag_ss.at[p, 1], ag_rs.at[p, 1], {"tp": mate})
                arrived(rows.at[p, (1 - yy) * 2 + 1 - core], ag_ss.at[p, 2], ag_rs.at[p, 2], {"tp": mate})
                arrived(sc_in.at[p], sc_ss.at[p], sc_rs.at[p], {"sp": peer(p)})

    def xs_across():
        arrived(xs.at[across], xs_ss.at[0], xs_rs.at[0], {"tp": across})
        send(xs.at[across], xs.at[across], xs_ss.at[2], xs_rs.at[2], {"tp": mate})

    def xs_rest():
        arrived(xs.at[mate], xs_ss.at[1], xs_rs.at[1], {"tp": mate})
        arrived(xs.at[(1 - yy) * 2 + 1 - core], xs_ss.at[2], xs_rs.at[2], {"tp": mate})
        for j in range(tps):
            rows[0, j] = dot(both[0:cap, :], xs[j]).astype(BF16)

    def weights_here():
        for load in loads[4:]:
            load.wait()

    def shared():
        for load in loads[1:4]:
            load.wait()
        g = sum(dot(xs[j], sg[j * DT:(j + 1) * DT, :]) for j in range(tps)) * scale
        u = sum(dot(xs[j], su[j * DT:(j + 1) * DT, :]) for j in range(tps)) * scale
        hs = (silu(g) * u).astype(BF16)
        for j in range(tps):
            s3[j] = dot(hs, sd[:, j * DT:(j + 1) * DT]).astype(BF16)
        scatter_start(s3, p3, r3_ss, r3_rs)

    def shared_across():
        scatter_across(s3, p3, q3, z3, r3_ss, r3_rs)

    def shared_end():
        hidden_ref[...] = hidden_ref[...] + scatter_end(s3, p3, z3, r3_ss, r3_rs).astype(BF16).astype(F32)

    FF = eg.shape[1]
    tile = 256 if FF % 256 == 0 else FF
    tiles = FF // tile

    def expert_up(gi, start=0, stop=tiles):
        ps = groups[gi]
        m = len(ps) * cap
        factors = []
        for p in ps:
            line = (sc_in if p else sc_out)[p]
            factors.append(jnp.broadcast_to(line, (128, 128)).T[0:cap, 0:1])
        factor = jnp.concatenate(factors, 0)
        span = pl.ds(ps[0] * cap, m)

        def up(i, _):
            cols = pl.ds(pl.multiple_of(i * tile, tile), tile)
            a = jnp.zeros((m, tile), F32)
            b = jnp.zeros((m, tile), F32)
            for j in range(tps):
                x = rows[ps[0]:ps[0] + len(ps), j].reshape(m, DT)
                a = a + dot(x, eg[j * DT:(j + 1) * DT, cols])
                b = b + dot(x, eu[j * DT:(j + 1) * DT, cols])
            hid[span, cols] = (silu(a * factor) * (b * factor)).astype(BF16)
            return 0

        lax.fori_loop(start, stop, up, 0)

    def expert_down(gi, half):
        span = span_of(gi)

        def down(j):
            s2[j, span] = dot(hid[span, :], ed[:, pl.ds(pl.multiple_of(j * DT, DT), DT)]).astype(BF16)

        for i, y2 in enumerate((1 - yy, yy)):
            if i in half:
                down(y2 * 2 + 1 - core)
                send(s2.at[y2 * 2 + 1 - core, span], p2.at[i, span], r2_ss.at[gi, i], r2_rs.at[gi, i], {"tp": mate})
                down(y2 * 2 + core)

    def span_of(gi):
        return pl.ds(groups[gi][0] * cap, len(groups[gi]) * cap)

    def scatter_sum(gi):
        span = span_of(gi)
        arrived(p2.at[0, span], r2_ss.at[gi, 0], r2_rs.at[gi, 0], {"tp": mate})
        q2[span] = (s2[across, span].astype(F32) + p2[0, span].astype(F32)).astype(BF16)

    def scatter_send(*ps):
        for p in ps:
            piece = pl.ds(p * cap, cap)
            send(q2.at[piece], z2.at[piece], q_ss.at[p], q_rs.at[p], {"tp": across})

    def mate_sum(gi):
        arrived(p2.at[1, span_of(gi)], r2_ss.at[gi, 1], r2_rs.at[gi, 1], {"tp": mate})

    def give_back(*ps):
        for p in ps:
            piece = pl.ds(p * cap, cap)
            arrived(z2.at[piece], q_ss.at[p], q_rs.at[p], {"tp": across})
            total = (s2[mt, piece].astype(F32) + p2[1, piece].astype(F32) + z2[piece].astype(F32)).astype(BF16)
            if p == 0:
                ret[piece] = total
            else:
                back[p] = total
                send(back.at[p], ret.at[piece], b_ss.at[p], b_rs.at[p], {"sp": peer(p)})

    def collect(gi):
        span = pl.ds(groups[gi][0] * cap, len(groups[gi]) * cap)
        for p in groups[gi]:
            if p:
                arrived(ret.at[pl.ds(p * cap, cap)], b_ss.at[p], b_rs.at[p], {"sp": peer(p)})
        total = hidden_ref[...]
        for k in range(2):
            weight = jnp.broadcast_to(weights_ref[k:k + 1, :], (R, R)).T[:, 0:1]
            chosen = lax.dot_general(
                sel[k, span], ret[span], (((0,), (0,)), ((), ())), preferred_element_type=F32)
            total = total + weight * chosen
        hidden_ref[...] = total

    forward_own(1)
    xs_across()
    forward_own(2)
    forward_across(1)
    xs_rest()
    forward_own(3)
    weights_here()
    all_here(0, 1)
    expert_up(0, 0, 2)
    forward_across(2)
    forward_own(4, 5)
    expert_up(0, 2, 4)
    expert_down(0, (0,))
    forward_own(6)
    expert_down(0, (1,))
    forward_across(3)
    shared()
    all_here(2, 3)
    expert_up(1, 0, 2)
    forward_own(7)
    forward_across(4)
    expert_up(1, 2, 4)
    forward_across(5)
    expert_down(1, (0, 1))
    all_here(4, 5)
    expert_up(2, 0, 1)
    scatter_sum(1)
    scatter_send(2, 3)
    forward_across(6)
    expert_up(2, 1, 2)
    forward_across(7)
    scatter_sum(0)
    scatter_send(1, 0)
    expert_up(2, 2, 3)
    all_here(6, 7)
    expert_up(3)
    mate_sum(1)
    give_back(2)
    expert_down(3, (0, 1))
    give_back(3)
    expert_up(2, 3, 4)
    scatter_sum(3)
    scatter_send(6, 7)
    expert_down(2, (0, 1))
    mate_sum(0)
    give_back(1)
    scatter_sum(2)
    scatter_send(4, 5)
    shared_across()
    mate_sum(3)
    give_back(6, 7)
    mate_sum(2)
    give_back(4, 5, 0)
    collect(0)
    collect(1)
    shared_end()
    collect(3)
    collect(2)
    out_ref[...] = hidden_ref[...].astype(BF16)
    for copy in sends:
        copy.wait_send()

    @pl.when(me < n - 1)
    def _():
        pltpu.make_async_remote_copy(
            src_ref=pool_ref.at[pl.ds(R - 16, 16)], dst_ref=halo_in,
            send_sem=halo_sem.at[0], recv_sem=halo_sem.at[1],
            device_id={"sp": following}, device_id_type=pl.DeviceIdType.MESH).wait_send()


def body(
    pool_input, doc_ids, residual, pool_gain, out_proj, norm_gain, routes, route_weights,
    expert_gate, expert_up, expert_down, shared_gate, shared_up, shared_down,
):
    n, tps = lax.axis_size("sp"), lax.axis_size("tp")
    R, C = pool_input.shape
    DT = residual.shape[1]
    FF, FS, D = expert_gate.shape[2], shared_gate.shape[1], expert_gate.shape[1]
    experts = expert_gate.shape[0] * n
    top = routes.shape[1]
    cap = tps * max(1, 2 * R * top // (experts * tps))
    groups = [[0, 1], [2, 3], [4, 5], [6, 7]]
    V, DMA = pltpu.VMEM, pltpu.SemaphoreType.DMA
    scratch = [
        V((R, C), BF16), V((1, R), jnp.int32), V((top, R), jnp.int32), V((top, R), F32),
        V((R, DT), BF16), V((1, C), F32), V((1, DT), F32), DMA((7,)),
        V((C, D), BF16), V((D, FF), BF16), V((D, FF), BF16), V((FF, D), BF16),
        V((D, FS), BF16), V((D, FS), BF16), V((FS, D), BF16), DMA((7,)),
        V((1, C + 256), F32), V((n, 1, C + 256), F32), V((16, C), BF16), DMA((n,)), DMA((n,)), DMA((2,)),
        V((tps, R, DT), BF16), V((2, R, DT), BF16), V((R, DT), BF16), V((R, DT), BF16), DMA((3,)), DMA((3,)),
        V((8, R), F32), V((tps, 8, R), F32), DMA((tps,)), DMA((tps,)),
        V((2, n * cap, R), BF16), V((n * cap, R), BF16), V((n, 1, 128), F32), V((n, 1, 128), F32), DMA((n,)), DMA((n,)),
        V((n, cap, DT), BF16), V((n, tps, cap, DT), BF16),
        DMA((n,)), DMA((n,)), DMA((n, 3)), DMA((n, 3)),
        V((R, DT), BF16), V((tps, R, DT), BF16), DMA((3,)), DMA((3,)),
        V((tps, R, DT), BF16), V((2, R, DT), BF16), V((R, DT), BF16), V((R, DT), BF16), DMA((3,)), DMA((3,)),
        V((n * cap, FF), BF16), V((tps, n * cap, DT), BF16), V((2, n * cap, DT), BF16),
        V((n * cap, DT), BF16), V((n * cap, DT), BF16), DMA((len(groups), 2)), DMA((len(groups), 2)), DMA((n,)), DMA((n,)),
        V((n, cap, DT), BF16), V((n * cap, DT), BF16), DMA((n,)), DMA((n,)),
        V((R, DT), F32),
    ]
    vm = pl.BlockSpec(memory_space=pltpu.VMEM)
    hb = pl.BlockSpec(memory_space=pltpu.HBM)
    return pl.pallas_call(
        functools.partial(layer_kernel, groups),
        out_shape=jax.ShapeDtypeStruct((R, DT), BF16),
        in_specs=[hb] * 14,
        out_specs=vm,
        scratch_shapes=scratch,
        compiler_params=pltpu.CompilerParams(
            collective_id=0, has_side_effects=True, vmem_limit_bytes=60 * 2**20),
    )(pool_input, doc_ids.reshape(1, R), routes.T, route_weights.T, residual, pool_gain.reshape(1, C), norm_gain.reshape(1, DT),
      out_proj, expert_gate, expert_up, expert_down, shared_gate, shared_up, shared_down)


def one_kernel_fits(mesh):
    return mesh.shape["tp"] == 4 and mesh.shape["sp"] == 8


def solution(mesh):
    placed = (
        P("sp", "tp"),
        P("sp"),
        P("sp", "tp"),
        P("tp"),
        P("tp", None),
        P("tp"),
        P("sp", None),
        P("sp", None),
        P("sp", None, "tp"),
        P("sp", None, "tp"),
        P("sp", "tp", None),
        P(None, "tp"),
        P(None, "tp"),
        P("tp", None),
    )
    return jax.shard_map(
        body if one_kernel_fits(mesh) else plain_body, mesh=mesh, in_specs=placed, out_specs=P("sp", "tp"), check_vma=False)
```

```python
import jax
import functools
import jax.numpy as jnp
from jax import lax
from jax.experimental import pallas as pl
from jax.experimental.pallas import tpu as pltpu
from jax.sharding import PartitionSpec as P


def carried_in(value, axis, join, neutral):
    count, mine = (lax.axis_size(axis), lax.axis_index(axis))
    pieces = jax.tree.map(lambda part: lax.all_gather(part, axis), value)
    subtotal = jax.tree.map(
        lambda part, zero: jnp.full_like(part, 0) + jnp.asarray(zero, part.dtype), value, neutral
    )

    def hop(position, subtotal):
        longer = join(subtotal, jax.tree.map(lambda part: part[position], pieces))
        return jax.tree.map(lambda new, old: jnp.where(position < mine, new, old), longer, subtotal)

    return lax.fori_loop(0, count - 1, hop, subtotal)


def from_behind(value, axis, by):
    size = lax.axis_size(axis)
    pairs = [(i, i + by) for i in range(size) if 0 <= i + by < size]
    return lax.ppermute(value, axis, pairs)


def join_documents(earlier, later):
    earlier_sum, earlier_length, earlier_first, earlier_last, earlier_inner = earlier
    later_sum, later_length, later_first, later_last, later_inner = later
    boundary = later_first != earlier_last
    restart = (later_inner > 0) | boundary
    merged = (
        jnp.where(restart, later_sum, earlier_sum + later_sum),
        jnp.where(restart, later_length, earlier_length + later_length),
        earlier_first,
        later_last,
        jnp.maximum(jnp.maximum(earlier_inner, later_inner), boundary.astype(jnp.float32)),
    )
    earlier_empty = earlier_first < 0
    later_empty = later_first < 0
    return tuple(
        (
            jnp.where(earlier_empty, second, jnp.where(later_empty, first_value, joined))
            for first_value, second, joined in zip(earlier, later, merged)
        )
    )


def expert_terms(arrived, gate_weight, up_weight, down_weight):
    local_experts = gate_weight.shape[0]
    sources = arrived.shape[0] // local_experts
    grouped = arrived.reshape(sources, local_experts, arrived.shape[1], arrived.shape[2])
    gate = jnp.einsum("secd,edf->secf", grouped, gate_weight, preferred_element_type=jnp.float32)
    upper = jnp.einsum("secd,edf->secf", grouped, up_weight, preferred_element_type=jnp.float32)
    hidden = (jax.nn.silu(gate) * upper).astype(jnp.bfloat16)
    output = jnp.einsum("secf,efd->secd", hidden, down_weight, preferred_element_type=jnp.float32)
    return output.reshape(arrived.shape[0], arrived.shape[1], down_weight.shape[2])


def plain_body(
    pool_input,
    doc_ids,
    residual,
    pool_gain,
    out_proj,
    norm_gain,
    routes,
    route_weights,
    expert_gate,
    expert_up,
    expert_down,
    shared_gate,
    shared_up,
    shared_down,
):
    row_count, channels = pool_input.shape
    values = pool_input.astype(jnp.float32)
    positions = jnp.arange(row_count, dtype=jnp.int32)
    inner_begin = jnp.concatenate([jnp.zeros((1,), bool), doc_ids[1:] != doc_ids[:-1]])
    running = jnp.cumsum(values[:, 3::4], axis=0)
    shifted = jnp.concatenate([jnp.zeros((1, running.shape[1]), jnp.float32), running], 0)
    inner_last = jnp.max(jnp.where(inner_begin, positions, 0))
    own_terms = (
        running[-1] - shifted[inner_last],
        (row_count - inner_last).astype(jnp.float32),
        doc_ids[0].astype(jnp.float32),
        doc_ids[-1].astype(jnp.float32),
        jnp.any(inner_begin).astype(jnp.float32),
    )
    identity = (
        jnp.zeros((running.shape[1],), jnp.float32),
        jnp.zeros((), jnp.float32),
        jnp.full((), -1.0, jnp.float32),
        jnp.full((), -1.0, jnp.float32),
        jnp.zeros((), jnp.float32),
    )
    before = carried_in(own_terms, "sp", join_documents, identity)
    fresh = (before[2] < 0) | (doc_ids[0].astype(jnp.float32) != before[3])
    begins = jnp.concatenate([fresh[None], inner_begin[1:]])
    doc_start = lax.cummax(jnp.where(begins, positions, -1), axis=0)
    found = doc_start >= 0
    carry_sum = jnp.where(fresh, 0.0, before[0])
    carry_length = jnp.where(fresh, 0.0, before[1])
    length = jnp.where(
        found,
        (positions - doc_start + 1).astype(jnp.float32),
        carry_length + (positions + 1).astype(jnp.float32),
    )
    start_rows = jnp.take(shifted, jnp.maximum(doc_start, 0), axis=0)
    doc_sum = jnp.where(found[:, None], running - start_rows, carry_sum[None, :] + running)
    doc_mean = doc_sum / length[:, None]
    rim = from_behind(pool_input[row_count - 15 :], "sp", 1)
    extended = jnp.concatenate([rim, pool_input], 0).astype(jnp.float32)
    scale_index = jnp.arange(channels, dtype=jnp.int32) % 4
    window_size = jnp.where(scale_index == 0, 2.0, jnp.where(scale_index == 1, 8.0, 16.0))
    window_total = jnp.zeros((row_count, channels), jnp.float32)
    for offset in range(16):
        inside = (offset < length[:, None]) & (offset < window_size[None, :])
        window_total = window_total + jnp.where(
            inside, extended[15 - offset : 15 - offset + row_count], 0.0
        )
    window_mean = window_total / jnp.minimum(length[:, None], window_size[None, :])
    pool_mean = jnp.concatenate(
        [window_mean.reshape(row_count, channels // 4, 4)[..., :3], doc_mean[..., None]], -1
    )
    pool_mean = pool_mean.reshape(row_count, channels)
    pooled = ((pool_mean - values) * pool_gain).astype(jnp.bfloat16)
    terms = jnp.dot(pooled, out_proj, preferred_element_type=jnp.float32)
    projected = lax.psum_scatter(terms.astype(jnp.bfloat16), "tp", scatter_dimension=1, tiled=True)
    hidden_state = residual.astype(jnp.float32) + projected.astype(jnp.float32)
    squares = lax.psum(jnp.sum(hidden_state * hidden_state, axis=1), "tp")
    model_width = residual.shape[1] * lax.axis_size("tp")
    scaling = lax.rsqrt(squares / model_width + 1e-06)
    normed_columns = (hidden_state * scaling[:, None] * norm_gain).astype(jnp.bfloat16)
    normed = lax.all_gather(normed_columns, "tp", axis=1, tiled=True)
    shared_gate_out = jnp.dot(normed, shared_gate, preferred_element_type=jnp.float32)
    shared_up_out = jnp.dot(normed, shared_up, preferred_element_type=jnp.float32)
    shared_hidden = (jax.nn.silu(shared_gate_out) * shared_up_out).astype(jnp.bfloat16)
    shared_terms = jnp.dot(shared_hidden, shared_down, preferred_element_type=jnp.float32)
    group_size = lax.axis_size("tp")
    experts = expert_gate.shape[0] * lax.axis_size("sp")
    top = routes.shape[1]
    capacity = group_size * max(1, 2 * row_count * top // (experts * group_size))
    flat_experts = routes.reshape(-1)
    onehot = (flat_experts[:, None] == jnp.arange(experts, dtype=jnp.int32)[None, :]).astype(
        jnp.int32
    )
    ranks = jnp.sum((jnp.cumsum(onehot, axis=0) - 1) * onehot, axis=1)
    slots = flat_experts * capacity + ranks
    token_index = jnp.arange(row_count * top, dtype=jnp.int32) // top
    slot_token = jnp.full((experts * capacity,), row_count, jnp.int32).at[slots].set(token_index)
    with_blank = jnp.concatenate([normed, jnp.zeros((1, normed.shape[1]), jnp.bfloat16)], 0)
    outgoing = jnp.take(with_blank, slot_token, axis=0).reshape(experts, capacity, normed.shape[1])
    share = capacity // group_size
    mine = lax.dynamic_slice_in_dim(outgoing, lax.axis_index("tp") * share, share, 1)
    arrived = lax.all_to_all(mine, "sp", split_axis=0, concat_axis=0, tiled=True)
    run_arrived = lax.all_gather(arrived, "tp", axis=1, tiled=True)
    expert_parts = expert_terms(run_arrived, expert_gate, expert_up, expert_down)
    routed_sum, shared_sum = (
        lax.psum_scatter(
            expert_parts.astype(jnp.bfloat16), "tp", scatter_dimension=2, tiled=True
        ).astype(jnp.float32),
        lax.psum_scatter(
            shared_terms[None].astype(jnp.bfloat16), "tp", scatter_dimension=2, tiled=True
        ).astype(jnp.float32),
    )
    returned = lax.all_to_all(
        routed_sum.astype(jnp.bfloat16), "sp", split_axis=0, concat_axis=0, tiled=True
    )
    flat_back = returned.reshape(experts * capacity, returned.shape[2])
    picked = (
        jnp.take(flat_back, slots, axis=0).astype(jnp.float32) * route_weights.reshape(-1)[:, None]
    )
    routed = jnp.sum(picked.reshape(row_count, top, flat_back.shape[1]), axis=1)
    shared_out = shared_sum[0].astype(jnp.bfloat16).astype(jnp.float32)
    return (hidden_state + routed + shared_out).astype(jnp.bfloat16)


F32 = jnp.float32
BF16 = jnp.bfloat16


def dot(a, b):
    return jnp.dot(a, b, preferred_element_type=F32)


def silu(v):
    return v * jax.nn.sigmoid(v)


def layer_kernel(
    groups,
    pool_hbm, doc_hbm, routes_hbm, weights_hbm, resid_hbm, gain_hbm, ngain_hbm, oproj_hbm, eg_hbm, eu_hbm, ed_hbm, sg_hbm, su_hbm, sd_hbm,
    out_ref,
    pool_ref, doc_ref, routes_ref, weights_ref, resid_ref, gain_ref, ngain_ref, isem,
    oproj, eg, eu, ed, sg, su, sd, wsem,
    stat_out, stat_in, halo_in, stat_ss, stat_rs, halo_sem,
    s1, p1, q1, z1, r1_ss, r1_rs,
    ss_out, ss_in, ss_ss, ss_rs,
    sel, both, sc_out, sc_in, sc_ss, sc_rs, disp, rows, d_ss, d_rs, ag_ss, ag_rs,
    normed_ref, xs, xs_ss, xs_rs,
    s3, p3, q3, z3, r3_ss, r3_rs,
    hid, s2, p2, q2, z2, r2_ss, r2_rs, q_ss, q_rs,
    back, ret, b_ss, b_rs,
    hidden_ref,
):
    n = lax.axis_size("sp")
    tps = lax.axis_size("tp")
    me = lax.axis_index("sp")
    mt = lax.axis_index("tp")
    core = lax.rem(mt, 2)
    yy = mt // 2
    mate = yy * 2 + (1 - core)
    across = (1 - yy) * 2 + core
    R, C = pool_ref.shape
    DT = resid_ref.shape[1]
    D = DT * tps
    cap = disp.shape[1]

    def key(p):
        return (p & 1) | ((p & 2) << 1) | ((p & 4) >> 1)

    def peer(p):
        return me ^ key(p)

    barrier = pltpu.get_barrier_semaphore()
    for k in range(1, n):
        pl.semaphore_signal(barrier, inc=1, device_id={"sp": peer(k)},
                            device_id_type=pl.DeviceIdType.MESH)
    for j in range(1, tps):
        pl.semaphore_signal(barrier, inc=1, device_id={"tp": lax.rem(mt + j, tps)},
                            device_id_type=pl.DeviceIdType.MESH)

    small = [
        pltpu.make_async_copy(src, dst, isem.at[i])
        for i, (src, dst) in enumerate((
            (doc_hbm, doc_ref), (pool_hbm, pool_ref), (routes_hbm, routes_ref), (gain_hbm, gain_ref),
            (resid_hbm, resid_ref), (ngain_hbm, ngain_ref), (weights_hbm, weights_ref)))
    ]
    loads = [
        pltpu.make_async_copy(src, dst, wsem.at[i])
        for i, (src, dst) in enumerate((
            (oproj_hbm, oproj), (sg_hbm, sg), (su_hbm, su), (sd_hbm, sd),
            (eg_hbm.at[0], eg), (eu_hbm.at[0], eu), (ed_hbm.at[0], ed)))
    ]
    for load in small + loads:
        load.start()
    sends = []

    def send(src, dst, ss, rs, where):
        copy = pltpu.make_async_remote_copy(
            src_ref=src, dst_ref=dst, send_sem=ss, recv_sem=rs,
            device_id=where, device_id_type=pl.DeviceIdType.MESH)
        copy.start()
        sends.append(copy)

    def arrived(ref, ss, rs, where):
        pltpu.make_async_remote_copy(
            src_ref=ref, dst_ref=ref, send_sem=ss, recv_sem=rs,
            device_id=where, device_id_type=pl.DeviceIdType.MESH).wait_recv()

    small[0].wait()
    small[1].wait()
    doc = doc_ref[...].astype(F32)
    first = jnp.min(doc, axis=1, keepdims=True)
    last = jnp.max(doc, axis=1, keepdims=True)
    pool = pool_ref[...]
    tail_mask = jnp.broadcast_to((doc == last).astype(F32), (8, R))
    stat_out[:, 0:C] = dot(tail_mask.astype(BF16), pool)[0:1]
    stat_out[:, C:C + 128] = jnp.broadcast_to(last, (1, 128))
    stat_out[:, C + 128:C + 256] = jnp.broadcast_to(jnp.sum(tail_mask[0:1], axis=1, keepdims=True), (1, 128))

    t_pos = lax.broadcasted_iota(jnp.int32, (R, R), 0)
    u_pos = lax.broadcasted_iota(jnp.int32, (R, R), 1)
    gap = t_pos - u_pos
    doc_row = jnp.broadcast_to(doc, (R, R))
    doc_col = doc_row.T

    pl.semaphore_wait(barrier, n - 1 + tps - 1)
    following = jnp.minimum(me + 1, n - 1)

    @pl.when(me < n - 1)
    def _():
        pltpu.make_async_remote_copy(
            src_ref=pool_ref.at[pl.ds(R - 16, 16)], dst_ref=halo_in,
            send_sem=halo_sem.at[0], recv_sem=halo_sem.at[1],
            device_id={"sp": following}, device_id_type=pl.DeviceIdType.MESH).start()

    for k in range(1, n):
        send(stat_out, stat_in.at[k], stat_ss.at[k], stat_rs.at[k], {"sp": peer(k)})

    same = (doc_col == doc_row) & (gap >= 0)
    length = jnp.sum(same.astype(F32), axis=1, keepdims=True)
    windows = (2, 8, 16)
    totals = [dot((same & (gap < w)).astype(F32).astype(BF16), pool) for w in windows]
    totals.append(dot(same.astype(F32).astype(BF16), pool))

    e_iota = lax.broadcasted_iota(jnp.int32, (n, R), 0)
    picked = (key(e_iota) ^ me).astype(F32)
    small[2].wait()
    routes = routes_ref[...].astype(F32)
    r0 = (jnp.broadcast_to(routes[0:1], (n, R)) == picked).astype(F32)
    r1 = (jnp.broadcast_to(routes[1:2], (n, R)) == picked).astype(F32)
    member = r0 + r1
    rank = dot(member.astype(BF16), (gap < 0).astype(F32).astype(BF16))
    slot = lax.broadcasted_iota(jnp.int32, (cap, R), 0).astype(F32)
    for p in range(n):
        here = (jnp.broadcast_to(rank[p:p + 1], (cap, R)) == slot).astype(F32)
        sel[0, p * cap:(p + 1) * cap, :] = (here * r0[p:p + 1]).astype(BF16)
        sel[1, p * cap:(p + 1) * cap, :] = (here * r1[p:p + 1]).astype(BF16)
        both[p * cap:(p + 1) * cap, :] = (here * member[p:p + 1]).astype(BF16)

    @pl.when(me > 0)
    def _():
        arrived(halo_in, halo_sem.at[0], halo_sem.at[1], {"sp": peer(1)})

    for k in range(1, n):
        arrived(stat_in.at[k], stat_ss.at[k], stat_rs.at[k], {"sp": peer(k)})
    carry = jnp.zeros((1, C), F32)
    carry_length = jnp.zeros((1, 1), F32)
    before = jnp.zeros((1, R), F32)
    for k in range(1, n):
        source = jnp.full((1, 128), peer(k), jnp.int32)
        use = (stat_in[k, :, C:C + 128] == jnp.broadcast_to(first, (1, 128))) & (source < me)
        tail = jnp.where(use, stat_in[k, :, C + 128:C + 256], 0.0)
        keep = jnp.concatenate([use.astype(F32)] * (C // 128), axis=1)
        carry = carry + keep * stat_in[k, :, 0:C]
        carry_length = carry_length + tail[:, 0:1]
        before = before + jnp.where(source == me - 1, tail, 0.0)
    in_first = (doc_col == first).astype(F32)[:, 0:1]
    length = length + in_first * carry_length
    reach = gap + 16
    halo_ok = (doc_col == first) & (u_pos.astype(F32) >= 16.0 - jnp.broadcast_to(before, (R, R)))
    halo = jnp.where(jnp.full(halo_in.shape, me, jnp.int32) > 0, halo_in[...].astype(F32), 0.0).astype(BF16)
    totals = [
        total + dot((halo_ok & (reach < w)).astype(F32)[:, 0:16].astype(BF16), halo)
        for total, w in zip(totals, windows)
    ] + [totals[3] + in_first * carry]
    lane = lax.rem(lax.broadcasted_iota(jnp.int32, (R, C), 1), 4)
    mean = totals[3] / length
    for i, w in enumerate(windows):
        mean = jnp.where(lane == i, totals[i] / jnp.minimum(length, float(w)), mean)
    small[3].wait()
    pooled = ((mean - pool.astype(F32)) * gain_ref[...]).astype(BF16)

    def scatter_start(s, p, ss, rs):
        for i, y2 in enumerate((1 - yy, yy)):
            send(s.at[y2 * 2 + 1 - core], p.at[i], ss.at[i], rs.at[i], {"tp": mate})

    def scatter_across(s, p, q, z, ss, rs):
        arrived(p.at[0], ss.at[0], rs.at[0], {"tp": mate})
        q[...] = (s[across].astype(F32) + p[0].astype(F32)).astype(BF16)
        send(q, z, ss.at[2], rs.at[2], {"tp": across})

    def scatter_end(s, p, z, ss, rs):
        arrived(p.at[1], ss.at[1], rs.at[1], {"tp": mate})
        own = s[mt].astype(F32) + p[1].astype(F32)
        arrived(z, ss.at[2], rs.at[2], {"tp": across})
        return own + z[...].astype(F32)

    loads[0].wait()
    for j in range(tps):
        s1[j] = dot(pooled, oproj[:, j * DT:(j + 1) * DT]).astype(BF16)
    scatter_start(s1, p1, r1_ss, r1_rs)
    halves = [slice(h * DT // 2, (h + 1) * DT // 2) for h in range(2)]
    arrived(p1.at[0], r1_ss.at[0], r1_rs.at[0], {"tp": mate})
    q1[...] = (s1[across].astype(F32) + p1[0].astype(F32)).astype(BF16)
    for h, part in enumerate(halves):
        send(q1.at[:, part], z1.at[:, part], r1_ss.at[2 + h], r1_rs.at[2 + h], {"tp": across})
    for load in small[4:]:
        load.wait()
    arrived(p1.at[1], r1_ss.at[1], r1_rs.at[1], {"tp": mate})
    hidden_ref[...] = resid_ref[...].astype(F32) + (s1[mt].astype(F32) + p1[1].astype(F32))

    def gather(p, count, part):
        slots = dot(both[p * cap:(p + count) * cap, :], normed_ref[:, part]).astype(BF16)
        disp[p:p + count, :, part] = slots.reshape(count, cap, slots.shape[1])

    def dispatch(*ps):
        for p in ps:
            send(disp.at[p], rows.at[p, mt], d_ss.at[p, 0], d_rs.at[p, 0], {"sp": peer(p)})

    partial = []
    for h, part in enumerate(halves):
        arrived(z1.at[:, part], r1_ss.at[2 + h], r1_rs.at[2 + h], {"tp": across})
        hidden = hidden_ref[:, part] + z1[:, part].astype(F32)
        normed_ref[:, part] = (hidden * ngain_ref[:, part]).astype(BF16)
        gather(1, 5, part)
        for p in (4, 5, 2, 3, 1):
            send(disp.at[p, :, part], rows.at[p, mt, :, part], d_ss.at[p, h], d_rs.at[p, h], {"sp": peer(p)})
        hidden_ref[:, part] = hidden
        partial.append(jnp.sum(hidden * hidden, axis=1, keepdims=True))
        if h:
            sq_row = jnp.broadcast_to(partial[0] + partial[1], (R, R)).T
            ss_out[...] = sq_row[0:8]
            for j in range(1, tps):
                send(ss_out, ss_in.at[j], ss_ss.at[j], ss_rs.at[j], {"tp": lax.rem(mt + j, tps)})
        send(normed_ref.at[:, part], xs.at[mt, :, part], xs_ss.at[3 * h], xs_rs.at[3 * h], {"tp": across})
        send(normed_ref.at[:, part], xs.at[mt, :, part], xs_ss.at[3 * h + 1], xs_rs.at[3 * h + 1], {"tp": mate})
    gather(6, 2, slice(0, DT))
    dispatch(6)
    xs[mt] = normed_ref[...]

    all_sq = sq_row[0:8]
    for j in range(1, tps):
        arrived(ss_in.at[j], ss_ss.at[j], ss_rs.at[j], {"tp": mt})
        all_sq = all_sq + ss_in[j]
    scale_row = lax.rsqrt(all_sq / D + 1e-06)
    high = scale_row.astype(BF16)
    rest = scale_row - high.astype(F32)
    middle = rest.astype(BF16)
    low = (rest - middle.astype(F32)).astype(BF16)
    turned = (((1,), (1,)), ((), ()))
    slot_scale = sum(
        lax.dot_general(part, both[...], turned, preferred_element_type=F32) for part in (high, middle, low))
    for p in range(n):
        sc_out[p, :, 0:cap] = slot_scale[0:1, p * cap:(p + 1) * cap]
    for p in (6, 7, 2, 3, 4, 5, 1):
        send(sc_out.at[p], sc_in.at[p], sc_ss.at[p], sc_rs.at[p], {"sp": peer(p)})
    dispatch(7)
    scale = jnp.broadcast_to(scale_row[0:1], (R, R)).T[:, 0:1]

    def own_here(p):
        if p < 6:
            for h, part in enumerate(halves):
                arrived(rows.at[p, mt, :, part], d_ss.at[p, h], d_rs.at[p, h], {"sp": peer(p)})
        else:
            arrived(rows.at[p, mt], d_ss.at[p, 0], d_rs.at[p, 0], {"sp": peer(p)})

    def forward_own(*ps):
        for p in ps:
            own_here(p)
            send(rows.at[p, mt], rows.at[p, mt], ag_ss.at[p, 0], ag_rs.at[p, 0], {"tp": across})
            send(rows.at[p, mt], rows.at[p, mt], ag_ss.at[p, 1], ag_rs.at[p, 1], {"tp": mate})

    def forward_across(*ps):
        for p in ps:
            arrived(rows.at[p, across], ag_ss.at[p, 0], ag_rs.at[p, 0], {"tp": across})
            send(rows.at[p, across], rows.at[p, across], ag_ss.at[p, 2], ag_rs.at[p, 2], {"tp": mate})

    def all_here(*ps):
        for p in ps:
            if p:
                arrived(rows.at[p, mate], ag_ss.at[p, 1], ag_rs.at[p, 1], {"tp": mate})
                arrived(rows.at[p, (1 - yy) * 2 + 1 - core], ag_ss.at[p, 2], ag_rs.at[p, 2], {"tp": mate})
                arrived(sc_in.at[p], sc_ss.at[p], sc_rs.at[p], {"sp": peer(p)})

    def xs_across():
        for h, part in enumerate(halves):
            arrived(xs.at[across, :, part], xs_ss.at[3 * h], xs_rs.at[3 * h], {"tp": across})
        send(xs.at[across], xs.at[across], xs_ss.at[2], xs_rs.at[2], {"tp": mate})

    def xs_rest():
        for h, part in enumerate(halves):
            arrived(xs.at[mate, :, part], xs_ss.at[3 * h + 1], xs_rs.at[3 * h + 1], {"tp": mate})
        arrived(xs.at[(1 - yy) * 2 + 1 - core], xs_ss.at[2], xs_rs.at[2], {"tp": mate})
        for j in range(tps):
            rows[0, j] = dot(both[0:cap, :], xs[j]).astype(BF16)

    def weights_here():
        for load in loads[4:]:
            load.wait()

    def shared():
        for load in loads[1:4]:
            load.wait()
        g = sum(dot(xs[j], sg[j * DT:(j + 1) * DT, :]) for j in range(tps)) * scale
        u = sum(dot(xs[j], su[j * DT:(j + 1) * DT, :]) for j in range(tps)) * scale
        hs = (silu(g) * u).astype(BF16)
        own = weights_ref[0:1, :] * r0[0:1] + weights_ref[1:2, :] * r1[0:1]
        own = jnp.broadcast_to(own, (R, R)).T[:, 0:1]
        for j in range(tps):
            routed = lax.dot_general(
                both[0:cap, :], s2[j, 0:cap], (((0,), (0,)), ((), ())), preferred_element_type=F32)
            s3[j] = (dot(hs, sd[:, j * DT:(j + 1) * DT]) + own * routed).astype(BF16)
        scatter_start(s3, p3, r3_ss, r3_rs)

    def shared_across():
        scatter_across(s3, p3, q3, z3, r3_ss, r3_rs)

    def shared_end():
        hidden_ref[...] = hidden_ref[...] + scatter_end(s3, p3, z3, r3_ss, r3_rs)

    FF = eg.shape[1]
    tile = 256 if FF % 256 == 0 else FF
    tiles = FF // tile

    def expert_up(gi, start=0, stop=tiles):
        ps = groups[gi]
        m = len(ps) * cap
        factors = []
        for p in ps:
            line = (sc_in if p else sc_out)[p]
            factors.append(jnp.broadcast_to(line, (128, 128)).T[0:cap, 0:1])
        factor = jnp.concatenate(factors, 0)
        span = pl.ds(ps[0] * cap, m)

        def up(i, _):
            cols = pl.ds(pl.multiple_of(i * tile, tile), tile)
            a = jnp.zeros((m, tile), F32)
            b = jnp.zeros((m, tile), F32)
            for j in range(tps):
                x = rows[ps[0]:ps[0] + len(ps), j].reshape(m, DT)
                a = a + dot(x, eg[j * DT:(j + 1) * DT, cols])
                b = b + dot(x, eu[j * DT:(j + 1) * DT, cols])
            hid[span, cols] = (silu(a * factor) * (b * factor)).astype(BF16)
            return 0

        lax.fori_loop(start, stop, up, 0)

    def expert_down(gi, half):
        span = span_of(gi)
        whole = pl.ds(groups[gi][0] * cap, len(groups[gi]) * cap)

        def down(j):
            s2[j, whole] = dot(hid[whole, :], ed[:, pl.ds(pl.multiple_of(j * DT, DT), DT)]).astype(BF16)

        for i, y2 in enumerate((1 - yy, yy)):
            if i in half:
                down(y2 * 2 + 1 - core)
                send(s2.at[y2 * 2 + 1 - core, span], p2.at[i, span], r2_ss.at[gi, i], r2_rs.at[gi, i], {"tp": mate})
                down(y2 * 2 + core)

    def span_of(gi):
        away = [p for p in groups[gi] if p]
        return pl.ds(away[0] * cap, len(away) * cap)

    def scatter_sum(gi):
        span = span_of(gi)
        arrived(p2.at[0, span], r2_ss.at[gi, 0], r2_rs.at[gi, 0], {"tp": mate})
        q2[span] = (s2[across, span].astype(F32) + p2[0, span].astype(F32)).astype(BF16)

    def scatter_send(*ps):
        for p in ps:
            piece = pl.ds(p * cap, cap)
            send(q2.at[piece], z2.at[piece], q_ss.at[p], q_rs.at[p], {"tp": across})

    def mate_sum(gi):
        arrived(p2.at[1, span_of(gi)], r2_ss.at[gi, 1], r2_rs.at[gi, 1], {"tp": mate})

    def give_back(*ps):
        for p in ps:
            piece = pl.ds(p * cap, cap)
            arrived(z2.at[piece], q_ss.at[p], q_rs.at[p], {"tp": across})
            total = (s2[mt, piece].astype(F32) + p2[1, piece].astype(F32) + z2[piece].astype(F32)).astype(BF16)
            back[p] = total
            send(back.at[p], ret.at[piece], b_ss.at[p], b_rs.at[p], {"sp": peer(p)})

    def collect(gi):
        span = span_of(gi)
        for p in groups[gi]:
            if p:
                arrived(ret.at[pl.ds(p * cap, cap)], b_ss.at[p], b_rs.at[p], {"sp": peer(p)})
        total = hidden_ref[...]
        for k in range(2):
            weight = jnp.broadcast_to(weights_ref[k:k + 1, :], (R, R)).T[:, 0:1]
            chosen = lax.dot_general(
                sel[k, span], ret[span], (((0,), (0,)), ((), ())), preferred_element_type=F32)
            total = total + weight * chosen
        hidden_ref[...] = total

    forward_own(1)
    xs_across()
    forward_own(2)
    forward_across(1)
    xs_rest()
    forward_own(3)
    weights_here()
    all_here(0, 1)
    expert_up(0, 0, 2)
    forward_across(2)
    forward_own(4, 5)
    expert_up(0, 2, 4)
    expert_down(0, (0,))
    forward_own(6)
    expert_down(0, (1,))
    forward_across(3)
    shared()
    forward_own(7)
    all_here(2, 3)
    expert_up(1, 0, 2)
    forward_across(4)
    expert_up(1, 2, 4)
    forward_across(5)
    expert_down(1, (0, 1))
    scatter_sum(1)
    scatter_send(2, 3)
    scatter_sum(0)
    scatter_send(1)
    forward_across(6, 7)
    all_here(4, 5)
    expert_up(2, 0, 2)
    all_here(6, 7)
    expert_up(3)
    mate_sum(1)
    give_back(2)
    expert_down(3, (0, 1))
    scatter_sum(3)
    scatter_send(6, 7)
    give_back(3)
    expert_up(2, 2, 4)
    expert_down(2, (0, 1))
    mate_sum(0)
    give_back(1)
    mate_sum(3)
    scatter_sum(2)
    scatter_send(4, 5)
    shared_across()
    give_back(6, 7)
    mate_sum(2)
    give_back(4, 5)
    collect(0)
    collect(1)
    shared_end()
    collect(3)
    collect(2)
    out_ref[...] = hidden_ref[...].astype(BF16)
    for copy in sends:
        copy.wait_send()

    @pl.when(me < n - 1)
    def _():
        pltpu.make_async_remote_copy(
            src_ref=pool_ref.at[pl.ds(R - 16, 16)], dst_ref=halo_in,
            send_sem=halo_sem.at[0], recv_sem=halo_sem.at[1],
            device_id={"sp": following}, device_id_type=pl.DeviceIdType.MESH).wait_send()


def body(
    pool_input, doc_ids, residual, pool_gain, out_proj, norm_gain, routes, route_weights,
    expert_gate, expert_up, expert_down, shared_gate, shared_up, shared_down,
):
    n, tps = lax.axis_size("sp"), lax.axis_size("tp")
    R, C = pool_input.shape
    DT = residual.shape[1]
    FF, FS, D = expert_gate.shape[2], shared_gate.shape[1], expert_gate.shape[1]
    experts = expert_gate.shape[0] * n
    top = routes.shape[1]
    cap = tps * max(1, 2 * R * top // (experts * tps))
    groups = [[0, 1], [2, 3], [4, 5], [6, 7]]
    V, DMA = pltpu.VMEM, pltpu.SemaphoreType.DMA
    scratch = [
        V((R, C), BF16), V((1, R), jnp.int32), V((top, R), jnp.int32), V((top, R), F32),
        V((R, DT), BF16), V((1, C), F32), V((1, DT), F32), DMA((7,)),
        V((C, D), BF16), V((D, FF), BF16), V((D, FF), BF16), V((FF, D), BF16),
        V((D, FS), BF16), V((D, FS), BF16), V((FS, D), BF16), DMA((7,)),
        V((1, C + 256), F32), V((n, 1, C + 256), F32), V((16, C), BF16), DMA((n,)), DMA((n,)), DMA((2,)),
        V((tps, R, DT), BF16), V((2, R, DT), BF16), V((R, DT), BF16), V((R, DT), BF16), DMA((4,)), DMA((4,)),
        V((8, R), F32), V((tps, 8, R), F32), DMA((tps,)), DMA((tps,)),
        V((2, n * cap, R), BF16), V((n * cap, R), BF16), V((n, 1, 128), F32), V((n, 1, 128), F32), DMA((n,)), DMA((n,)),
        V((n, cap, DT), BF16), V((n, tps, cap, DT), BF16),
        DMA((n, 2)), DMA((n, 2)), DMA((n, 3)), DMA((n, 3)),
        V((R, DT), BF16), V((tps, R, DT), BF16), DMA((5,)), DMA((5,)),
        V((tps, R, DT), BF16), V((2, R, DT), BF16), V((R, DT), BF16), V((R, DT), BF16), DMA((3,)), DMA((3,)),
        V((n * cap, FF), BF16), V((tps, n * cap, DT), BF16), V((2, n * cap, DT), BF16),
        V((n * cap, DT), BF16), V((n * cap, DT), BF16), DMA((len(groups), 2)), DMA((len(groups), 2)), DMA((n,)), DMA((n,)),
        V((n, cap, DT), BF16), V((n * cap, DT), BF16), DMA((n,)), DMA((n,)),
        V((R, DT), F32),
    ]
    vm = pl.BlockSpec(memory_space=pltpu.VMEM)
    hb = pl.BlockSpec(memory_space=pltpu.HBM)
    return pl.pallas_call(
        functools.partial(layer_kernel, groups),
        out_shape=pltpu.VMEM((R, DT), BF16),
        in_specs=[hb] * 14,
        out_specs=vm,
        scratch_shapes=scratch,
        compiler_params=pltpu.CompilerParams(
            collective_id=0, has_side_effects=True, vmem_limit_bytes=60 * 2**20),
    )(pool_input, doc_ids.reshape(1, R), routes.T, route_weights.T, residual, pool_gain.reshape(1, C), norm_gain.reshape(1, DT),
      out_proj, expert_gate, expert_up, expert_down, shared_gate, shared_up, shared_down)


def one_kernel_fits(mesh):
    return mesh.shape["tp"] == 4 and mesh.shape["sp"] == 8


def solution(mesh):
    placed = (
        P("sp", "tp"),
        P("sp"),
        P("sp", "tp"),
        P("tp"),
        P("tp", None),
        P("tp"),
        P("sp", None),
        P("sp", None),
        P("sp", None, "tp"),
        P("sp", None, "tp"),
        P("sp", "tp", None),
        P(None, "tp"),
        P(None, "tp"),
        P("tp", None),
    )
    return jax.shard_map(
        body if one_kernel_fits(mesh) else plain_body, mesh=mesh, in_specs=placed, out_specs=P("sp", "tp"), check_vma=False)
```

```python
import jax
import functools
import jax.numpy as jnp
from jax import lax
from jax.experimental import pallas as pl
from jax.experimental.pallas import tpu as pltpu
from jax.sharding import PartitionSpec as P


def carried_in(value, axis, join, neutral):
    count, mine = (lax.axis_size(axis), lax.axis_index(axis))
    pieces = jax.tree.map(lambda part: lax.all_gather(part, axis), value)
    subtotal = jax.tree.map(
        lambda part, zero: jnp.full_like(part, 0) + jnp.asarray(zero, part.dtype), value, neutral
    )

    def hop(position, subtotal):
        longer = join(subtotal, jax.tree.map(lambda part: part[position], pieces))
        return jax.tree.map(lambda new, old: jnp.where(position < mine, new, old), longer, subtotal)

    return lax.fori_loop(0, count - 1, hop, subtotal)


def from_behind(value, axis, by):
    size = lax.axis_size(axis)
    pairs = [(i, i + by) for i in range(size) if 0 <= i + by < size]
    return lax.ppermute(value, axis, pairs)


def join_documents(earlier, later):
    earlier_sum, earlier_length, earlier_first, earlier_last, earlier_inner = earlier
    later_sum, later_length, later_first, later_last, later_inner = later
    boundary = later_first != earlier_last
    restart = (later_inner > 0) | boundary
    merged = (
        jnp.where(restart, later_sum, earlier_sum + later_sum),
        jnp.where(restart, later_length, earlier_length + later_length),
        earlier_first,
        later_last,
        jnp.maximum(jnp.maximum(earlier_inner, later_inner), boundary.astype(jnp.float32)),
    )
    earlier_empty = earlier_first < 0
    later_empty = later_first < 0
    return tuple(
        (
            jnp.where(earlier_empty, second, jnp.where(later_empty, first_value, joined))
            for first_value, second, joined in zip(earlier, later, merged)
        )
    )


def expert_terms(arrived, gate_weight, up_weight, down_weight):
    local_experts = gate_weight.shape[0]
    sources = arrived.shape[0] // local_experts
    grouped = arrived.reshape(sources, local_experts, arrived.shape[1], arrived.shape[2])
    gate = jnp.einsum("secd,edf->secf", grouped, gate_weight, preferred_element_type=jnp.float32)
    upper = jnp.einsum("secd,edf->secf", grouped, up_weight, preferred_element_type=jnp.float32)
    hidden = (jax.nn.silu(gate) * upper).astype(jnp.bfloat16)
    output = jnp.einsum("secf,efd->secd", hidden, down_weight, preferred_element_type=jnp.float32)
    return output.reshape(arrived.shape[0], arrived.shape[1], down_weight.shape[2])


def plain_body(
    pool_input,
    doc_ids,
    residual,
    pool_gain,
    out_proj,
    norm_gain,
    routes,
    route_weights,
    expert_gate,
    expert_up,
    expert_down,
    shared_gate,
    shared_up,
    shared_down,
):
    row_count, channels = pool_input.shape
    values = pool_input.astype(jnp.float32)
    positions = jnp.arange(row_count, dtype=jnp.int32)
    inner_begin = jnp.concatenate([jnp.zeros((1,), bool), doc_ids[1:] != doc_ids[:-1]])
    running = jnp.cumsum(values[:, 3::4], axis=0)
    shifted = jnp.concatenate([jnp.zeros((1, running.shape[1]), jnp.float32), running], 0)
    inner_last = jnp.max(jnp.where(inner_begin, positions, 0))
    own_terms = (
        running[-1] - shifted[inner_last],
        (row_count - inner_last).astype(jnp.float32),
        doc_ids[0].astype(jnp.float32),
        doc_ids[-1].astype(jnp.float32),
        jnp.any(inner_begin).astype(jnp.float32),
    )
    identity = (
        jnp.zeros((running.shape[1],), jnp.float32),
        jnp.zeros((), jnp.float32),
        jnp.full((), -1.0, jnp.float32),
        jnp.full((), -1.0, jnp.float32),
        jnp.zeros((), jnp.float32),
    )
    before = carried_in(own_terms, "sp", join_documents, identity)
    fresh = (before[2] < 0) | (doc_ids[0].astype(jnp.float32) != before[3])
    begins = jnp.concatenate([fresh[None], inner_begin[1:]])
    doc_start = lax.cummax(jnp.where(begins, positions, -1), axis=0)
    found = doc_start >= 0
    carry_sum = jnp.where(fresh, 0.0, before[0])
    carry_length = jnp.where(fresh, 0.0, before[1])
    length = jnp.where(
        found,
        (positions - doc_start + 1).astype(jnp.float32),
        carry_length + (positions + 1).astype(jnp.float32),
    )
    start_rows = jnp.take(shifted, jnp.maximum(doc_start, 0), axis=0)
    doc_sum = jnp.where(found[:, None], running - start_rows, carry_sum[None, :] + running)
    doc_mean = doc_sum / length[:, None]
    rim = from_behind(pool_input[row_count - 15 :], "sp", 1)
    extended = jnp.concatenate([rim, pool_input], 0).astype(jnp.float32)
    scale_index = jnp.arange(channels, dtype=jnp.int32) % 4
    window_size = jnp.where(scale_index == 0, 2.0, jnp.where(scale_index == 1, 8.0, 16.0))
    window_total = jnp.zeros((row_count, channels), jnp.float32)
    for offset in range(16):
        inside = (offset < length[:, None]) & (offset < window_size[None, :])
        window_total = window_total + jnp.where(
            inside, extended[15 - offset : 15 - offset + row_count], 0.0
        )
    window_mean = window_total / jnp.minimum(length[:, None], window_size[None, :])
    pool_mean = jnp.concatenate(
        [window_mean.reshape(row_count, channels // 4, 4)[..., :3], doc_mean[..., None]], -1
    )
    pool_mean = pool_mean.reshape(row_count, channels)
    pooled = ((pool_mean - values) * pool_gain).astype(jnp.bfloat16)
    terms = jnp.dot(pooled, out_proj, preferred_element_type=jnp.float32)
    projected = lax.psum_scatter(terms.astype(jnp.bfloat16), "tp", scatter_dimension=1, tiled=True)
    hidden_state = residual.astype(jnp.float32) + projected.astype(jnp.float32)
    squares = lax.psum(jnp.sum(hidden_state * hidden_state, axis=1), "tp")
    model_width = residual.shape[1] * lax.axis_size("tp")
    scaling = lax.rsqrt(squares / model_width + 1e-06)
    normed_columns = (hidden_state * scaling[:, None] * norm_gain).astype(jnp.bfloat16)
    normed = lax.all_gather(normed_columns, "tp", axis=1, tiled=True)
    shared_gate_out = jnp.dot(normed, shared_gate, preferred_element_type=jnp.float32)
    shared_up_out = jnp.dot(normed, shared_up, preferred_element_type=jnp.float32)
    shared_hidden = (jax.nn.silu(shared_gate_out) * shared_up_out).astype(jnp.bfloat16)
    shared_terms = jnp.dot(shared_hidden, shared_down, preferred_element_type=jnp.float32)
    group_size = lax.axis_size("tp")
    experts = expert_gate.shape[0] * lax.axis_size("sp")
    top = routes.shape[1]
    capacity = group_size * max(1, 2 * row_count * top // (experts * group_size))
    flat_experts = routes.reshape(-1)
    onehot = (flat_experts[:, None] == jnp.arange(experts, dtype=jnp.int32)[None, :]).astype(
        jnp.int32
    )
    ranks = jnp.sum((jnp.cumsum(onehot, axis=0) - 1) * onehot, axis=1)
    slots = flat_experts * capacity + ranks
    token_index = jnp.arange(row_count * top, dtype=jnp.int32) // top
    slot_token = jnp.full((experts * capacity,), row_count, jnp.int32).at[slots].set(token_index)
    with_blank = jnp.concatenate([normed, jnp.zeros((1, normed.shape[1]), jnp.bfloat16)], 0)
    outgoing = jnp.take(with_blank, slot_token, axis=0).reshape(experts, capacity, normed.shape[1])
    share = capacity // group_size
    mine = lax.dynamic_slice_in_dim(outgoing, lax.axis_index("tp") * share, share, 1)
    arrived = lax.all_to_all(mine, "sp", split_axis=0, concat_axis=0, tiled=True)
    run_arrived = lax.all_gather(arrived, "tp", axis=1, tiled=True)
    expert_parts = expert_terms(run_arrived, expert_gate, expert_up, expert_down)
    routed_sum, shared_sum = (
        lax.psum_scatter(
            expert_parts.astype(jnp.bfloat16), "tp", scatter_dimension=2, tiled=True
        ).astype(jnp.float32),
        lax.psum_scatter(
            shared_terms[None].astype(jnp.bfloat16), "tp", scatter_dimension=2, tiled=True
        ).astype(jnp.float32),
    )
    returned = lax.all_to_all(
        routed_sum.astype(jnp.bfloat16), "sp", split_axis=0, concat_axis=0, tiled=True
    )
    flat_back = returned.reshape(experts * capacity, returned.shape[2])
    picked = (
        jnp.take(flat_back, slots, axis=0).astype(jnp.float32) * route_weights.reshape(-1)[:, None]
    )
    routed = jnp.sum(picked.reshape(row_count, top, flat_back.shape[1]), axis=1)
    shared_out = shared_sum[0].astype(jnp.bfloat16).astype(jnp.float32)
    return (hidden_state + routed + shared_out).astype(jnp.bfloat16)


F32 = jnp.float32
BF16 = jnp.bfloat16


def dot(a, b):
    return jnp.dot(a, b, preferred_element_type=F32)


def silu(v):
    return v * jax.nn.sigmoid(v)


def layer_kernel(
    groups,
    pool_hbm, doc_hbm, routes_hbm, weights_hbm, resid_hbm, gain_hbm, ngain_hbm, oproj_hbm, eg_hbm, eu_hbm, ed_hbm, sg_hbm, su_hbm, sd_hbm,
    out_ref,
    pool_ref, doc_ref, routes_ref, weights_ref, resid_ref, gain_ref, ngain_ref, isem,
    oproj, eg, eu, ed, sg, su, sd, wsem,
    stat_out, stat_in, halo_in, stat_ss, stat_rs, halo_sem,
    s1, p1, q1, z1, r1_ss, r1_rs,
    ss_out, ss_in, ss_ss, ss_rs,
    sel, both, sc_out, sc_in, sc_ss, sc_rs, disp, rows, d_ss, d_rs, ag_ss, ag_rs,
    normed_ref, xs, xs_ss, xs_rs,
    s3, p3, q3, z3, r3_ss, r3_rs,
    hid, s2, p2, q2, z2, r2_ss, r2_rs, q_ss, q_rs,
    back, ret, b_ss, b_rs,
    hidden_ref,
):
    n = lax.axis_size("sp")
    tps = lax.axis_size("tp")
    me = lax.axis_index("sp")
    mt = lax.axis_index("tp")
    core = lax.rem(mt, 2)
    yy = mt // 2
    mate = yy * 2 + (1 - core)
    across = (1 - yy) * 2 + core
    R, C = pool_ref.shape
    DT = resid_ref.shape[1]
    D = DT * tps
    cap = disp.shape[1]

    def key(p):
        return (p & 1) | ((p & 2) << 1) | ((p & 4) >> 1)

    def peer(p):
        return me ^ key(p)

    barrier = pltpu.get_barrier_semaphore()
    for k in range(1, n):
        pl.semaphore_signal(barrier, inc=1, device_id={"sp": peer(k)},
                            device_id_type=pl.DeviceIdType.MESH)
    for j in range(1, tps):
        pl.semaphore_signal(barrier, inc=1, device_id={"tp": lax.rem(mt + j, tps)},
                            device_id_type=pl.DeviceIdType.MESH)

    small = [
        pltpu.make_async_copy(src, dst, isem.at[i])
        for i, (src, dst) in enumerate((
            (doc_hbm, doc_ref), (pool_hbm, pool_ref), (routes_hbm, routes_ref), (gain_hbm, gain_ref),
            (resid_hbm, resid_ref), (ngain_hbm, ngain_ref), (weights_hbm, weights_ref)))
    ]
    loads = [
        pltpu.make_async_copy(src, dst, wsem.at[i])
        for i, (src, dst) in enumerate((
            (oproj_hbm, oproj), (sg_hbm, sg), (su_hbm, su), (sd_hbm, sd),
            (eg_hbm.at[0], eg), (eu_hbm.at[0], eu), (ed_hbm.at[0], ed)))
    ]
    for load in small + loads:
        load.start()
    sends = []

    def send(src, dst, ss, rs, where):
        copy = pltpu.make_async_remote_copy(
            src_ref=src, dst_ref=dst, send_sem=ss, recv_sem=rs,
            device_id=where, device_id_type=pl.DeviceIdType.MESH)
        copy.start()
        sends.append(copy)

    def arrived(ref, ss, rs, where):
        pltpu.make_async_remote_copy(
            src_ref=ref, dst_ref=ref, send_sem=ss, recv_sem=rs,
            device_id=where, device_id_type=pl.DeviceIdType.MESH).wait_recv()

    small[0].wait()
    small[1].wait()
    doc = doc_ref[...].astype(F32)
    first = jnp.min(doc, axis=1, keepdims=True)
    last = jnp.max(doc, axis=1, keepdims=True)
    pool = pool_ref[...]
    tail_mask = jnp.broadcast_to((doc == last).astype(F32), (8, R))
    stat_out[:, 0:C] = dot(tail_mask.astype(BF16), pool)[0:1]
    stat_out[:, C:C + 128] = jnp.broadcast_to(last, (1, 128))
    stat_out[:, C + 128:C + 256] = jnp.broadcast_to(jnp.sum(tail_mask[0:1], axis=1, keepdims=True), (1, 128))

    t_pos = lax.broadcasted_iota(jnp.int32, (R, R), 0)
    u_pos = lax.broadcasted_iota(jnp.int32, (R, R), 1)
    gap = t_pos - u_pos
    doc_row = jnp.broadcast_to(doc, (R, R))
    doc_col = doc_row.T

    pl.semaphore_wait(barrier, n - 1 + tps - 1)
    following = jnp.minimum(me + 1, n - 1)

    @pl.when(me < n - 1)
    def _():
        pltpu.make_async_remote_copy(
            src_ref=pool_ref.at[pl.ds(R - 16, 16)], dst_ref=halo_in,
            send_sem=halo_sem.at[0], recv_sem=halo_sem.at[1],
            device_id={"sp": following}, device_id_type=pl.DeviceIdType.MESH).start()

    for k in range(1, n):
        send(stat_out, stat_in.at[k], stat_ss.at[k], stat_rs.at[k], {"sp": peer(k)})

    same = (doc_col == doc_row) & (gap >= 0)
    length = jnp.sum(same.astype(F32), axis=1, keepdims=True)
    windows = (2, 8, 16)
    totals = [dot((same & (gap < w)).astype(F32).astype(BF16), pool) for w in windows]
    totals.append(dot(same.astype(F32).astype(BF16), pool))

    e_iota = lax.broadcasted_iota(jnp.int32, (n, R), 0)
    picked = (key(e_iota) ^ me).astype(F32)
    small[2].wait()
    routes = routes_ref[...].astype(F32)
    r0 = (jnp.broadcast_to(routes[0:1], (n, R)) == picked).astype(F32)
    r1 = (jnp.broadcast_to(routes[1:2], (n, R)) == picked).astype(F32)
    member = r0 + r1
    rank = dot(member.astype(BF16), (gap < 0).astype(F32).astype(BF16))
    slot = lax.broadcasted_iota(jnp.int32, (cap, R), 0).astype(F32)
    for p in range(n):
        here = (jnp.broadcast_to(rank[p:p + 1], (cap, R)) == slot).astype(F32)
        sel[0, p * cap:(p + 1) * cap, :] = (here * r0[p:p + 1]).astype(BF16)
        sel[1, p * cap:(p + 1) * cap, :] = (here * r1[p:p + 1]).astype(BF16)
        both[p * cap:(p + 1) * cap, :] = (here * member[p:p + 1]).astype(BF16)

    @pl.when(me > 0)
    def _():
        arrived(halo_in, halo_sem.at[0], halo_sem.at[1], {"sp": peer(1)})

    for k in range(1, n):
        arrived(stat_in.at[k], stat_ss.at[k], stat_rs.at[k], {"sp": peer(k)})
    carry = jnp.zeros((1, C), F32)
    carry_length = jnp.zeros((1, 1), F32)
    before = jnp.zeros((1, R), F32)
    for k in range(1, n):
        source = jnp.full((1, 128), peer(k), jnp.int32)
        use = (stat_in[k, :, C:C + 128] == jnp.broadcast_to(first, (1, 128))) & (source < me)
        tail = jnp.where(use, stat_in[k, :, C + 128:C + 256], 0.0)
        keep = jnp.concatenate([use.astype(F32)] * (C // 128), axis=1)
        carry = carry + keep * stat_in[k, :, 0:C]
        carry_length = carry_length + tail[:, 0:1]
        before = before + jnp.where(source == me - 1, tail, 0.0)
    in_first = (doc_col == first).astype(F32)[:, 0:1]
    length = length + in_first * carry_length
    reach = gap + 16
    halo_ok = (doc_col == first) & (u_pos.astype(F32) >= 16.0 - jnp.broadcast_to(before, (R, R)))
    halo = jnp.where(jnp.full(halo_in.shape, me, jnp.int32) > 0, halo_in[...].astype(F32), 0.0).astype(BF16)
    totals = [
        total + dot((halo_ok & (reach < w)).astype(F32)[:, 0:16].astype(BF16), halo)
        for total, w in zip(totals, windows)
    ] + [totals[3] + in_first * carry]
    lane = lax.rem(lax.broadcasted_iota(jnp.int32, (R, C), 1), 4)
    mean = totals[3] / length
    for i, w in enumerate(windows):
        mean = jnp.where(lane == i, totals[i] / jnp.minimum(length, float(w)), mean)
    small[3].wait()
    pooled = ((mean - pool.astype(F32)) * gain_ref[...]).astype(BF16)

    def scatter_start(s, p, ss, rs):
        for i, y2 in enumerate((1 - yy, yy)):
            send(s.at[y2 * 2 + 1 - core], p.at[i], ss.at[i], rs.at[i], {"tp": mate})

    def scatter_across(s, p, q, z, ss, rs):
        arrived(p.at[0], ss.at[0], rs.at[0], {"tp": mate})
        q[...] = (s[across].astype(F32) + p[0].astype(F32)).astype(BF16)
        send(q, z, ss.at[2], rs.at[2], {"tp": across})

    def scatter_end(s, p, z, ss, rs):
        arrived(p.at[1], ss.at[1], rs.at[1], {"tp": mate})
        own = s[mt].astype(F32) + p[1].astype(F32)
        arrived(z, ss.at[2], rs.at[2], {"tp": across})
        return own + z[...].astype(F32)

    loads[0].wait()
    for j in range(tps):
        s1[j] = dot(pooled, oproj[:, j * DT:(j + 1) * DT]).astype(BF16)
    scatter_start(s1, p1, r1_ss, r1_rs)
    halves = [slice(h * DT // 2, (h + 1) * DT // 2) for h in range(2)]
    arrived(p1.at[0], r1_ss.at[0], r1_rs.at[0], {"tp": mate})
    q1[...] = (s1[across].astype(F32) + p1[0].astype(F32)).astype(BF16)
    for h, part in enumerate(halves):
        send(q1.at[:, part], z1.at[:, part], r1_ss.at[2 + h], r1_rs.at[2 + h], {"tp": across})
    for load in small[4:]:
        load.wait()
    arrived(p1.at[1], r1_ss.at[1], r1_rs.at[1], {"tp": mate})
    hidden_ref[...] = resid_ref[...].astype(F32) + (s1[mt].astype(F32) + p1[1].astype(F32))

    def gather(p, count, part):
        slots = dot(both[p * cap:(p + count) * cap, :], normed_ref[:, part]).astype(BF16)
        disp[p:p + count, :, part] = slots.reshape(count, cap, slots.shape[1])

    def dispatch(*ps):
        for p in ps:
            send(disp.at[p], rows.at[p, mt], d_ss.at[p, 0], d_rs.at[p, 0], {"sp": peer(p)})

    partial = []
    for h, part in enumerate(halves):
        arrived(z1.at[:, part], r1_ss.at[2 + h], r1_rs.at[2 + h], {"tp": across})
        hidden = hidden_ref[:, part] + z1[:, part].astype(F32)
        normed_ref[:, part] = (hidden * ngain_ref[:, part]).astype(BF16)
        gather(1, 5, part)
        for p in (1, 2, 4, 3, 5):
            send(disp.at[p, :, part], rows.at[p, mt, :, part], d_ss.at[p, h], d_rs.at[p, h], {"sp": peer(p)})
        hidden_ref[:, part] = hidden
        partial.append(jnp.sum(hidden * hidden, axis=1, keepdims=True))
        if h:
            sq_row = jnp.broadcast_to(partial[0] + partial[1], (R, R)).T
            ss_out[...] = sq_row[0:8]
            for j in range(1, tps):
                send(ss_out, ss_in.at[j], ss_ss.at[j], ss_rs.at[j], {"tp": lax.rem(mt + j, tps)})
        send(normed_ref.at[:, part], xs.at[mt, :, part], xs_ss.at[3 * h], xs_rs.at[3 * h], {"tp": across})
        send(normed_ref.at[:, part], xs.at[mt, :, part], xs_ss.at[3 * h + 1], xs_rs.at[3 * h + 1], {"tp": mate})
    gather(6, 2, slice(0, DT))
    dispatch(6)
    xs[mt] = normed_ref[...]

    all_sq = sq_row[0:8]
    for j in range(1, tps):
        arrived(ss_in.at[j], ss_ss.at[j], ss_rs.at[j], {"tp": mt})
        all_sq = all_sq + ss_in[j]
    scale_row = lax.rsqrt(all_sq / D + 1e-06)
    high = scale_row.astype(BF16)
    rest = scale_row - high.astype(F32)
    middle = rest.astype(BF16)
    low = (rest - middle.astype(F32)).astype(BF16)
    turned = (((1,), (1,)), ((), ()))
    slot_scale = sum(
        lax.dot_general(part, both[...], turned, preferred_element_type=F32) for part in (high, middle, low))
    for p in range(n):
        sc_out[p, :, 0:cap] = slot_scale[0:1, p * cap:(p + 1) * cap]
    for p in (6, 7, 2, 3, 4, 5, 1):
        send(sc_out.at[p], sc_in.at[p], sc_ss.at[p], sc_rs.at[p], {"sp": peer(p)})
    dispatch(7)
    scale = jnp.broadcast_to(scale_row[0:1], (R, R)).T[:, 0:1]

    def own_here(p):
        if p < 6:
            for h, part in enumerate(halves):
                arrived(rows.at[p, mt, :, part], d_ss.at[p, h], d_rs.at[p, h], {"sp": peer(p)})
        else:
            arrived(rows.at[p, mt], d_ss.at[p, 0], d_rs.at[p, 0], {"sp": peer(p)})

    def forward_own(*ps):
        for p in ps:
            own_here(p)
            send(rows.at[p, mt], rows.at[p, mt], ag_ss.at[p, 0], ag_rs.at[p, 0], {"tp": across})
            send(rows.at[p, mt], rows.at[p, mt], ag_ss.at[p, 1], ag_rs.at[p, 1], {"tp": mate})

    def forward_across(*ps):
        for p in ps:
            arrived(rows.at[p, across], ag_ss.at[p, 0], ag_rs.at[p, 0], {"tp": across})
            send(rows.at[p, across], rows.at[p, across], ag_ss.at[p, 2], ag_rs.at[p, 2], {"tp": mate})

    def all_here(*ps):
        for p in ps:
            if p:
                arrived(rows.at[p, mate], ag_ss.at[p, 1], ag_rs.at[p, 1], {"tp": mate})
                arrived(rows.at[p, (1 - yy) * 2 + 1 - core], ag_ss.at[p, 2], ag_rs.at[p, 2], {"tp": mate})
                arrived(sc_in.at[p], sc_ss.at[p], sc_rs.at[p], {"sp": peer(p)})

    def xs_across():
        for h, part in enumerate(halves):
            arrived(xs.at[across, :, part], xs_ss.at[3 * h], xs_rs.at[3 * h], {"tp": across})
        send(xs.at[across], xs.at[across], xs_ss.at[2], xs_rs.at[2], {"tp": mate})

    def xs_rest():
        for h, part in enumerate(halves):
            arrived(xs.at[mate, :, part], xs_ss.at[3 * h + 1], xs_rs.at[3 * h + 1], {"tp": mate})
        arrived(xs.at[(1 - yy) * 2 + 1 - core], xs_ss.at[2], xs_rs.at[2], {"tp": mate})
        for j in range(tps):
            rows[0, j] = dot(both[0:cap, :], xs[j]).astype(BF16)

    def weights_here():
        for load in loads[4:]:
            load.wait()

    def shared():
        for load in loads[1:4]:
            load.wait()
        g = sum(dot(xs[j], sg[j * DT:(j + 1) * DT, :]) for j in range(tps)) * scale
        u = sum(dot(xs[j], su[j * DT:(j + 1) * DT, :]) for j in range(tps)) * scale
        hs = (silu(g) * u).astype(BF16)
        own = weights_ref[0:1, :] * r0[0:1] + weights_ref[1:2, :] * r1[0:1]
        own = jnp.broadcast_to(own, (R, R)).T[:, 0:1]
        for j in range(tps):
            routed = lax.dot_general(
                both[0:cap, :], s2[j, 0:cap], (((0,), (0,)), ((), ())), preferred_element_type=F32)
            s3[j] = (dot(hs, sd[:, j * DT:(j + 1) * DT]) + own * routed).astype(BF16)
        scatter_start(s3, p3, r3_ss, r3_rs)

    def shared_across():
        scatter_across(s3, p3, q3, z3, r3_ss, r3_rs)

    def shared_end():
        hidden_ref[...] = hidden_ref[...] + scatter_end(s3, p3, z3, r3_ss, r3_rs)

    FF = eg.shape[1]
    tile = 256 if FF % 256 == 0 else FF
    tiles = FF // tile

    def expert_up(gi, start=0, stop=tiles):
        ps = groups[gi]
        m = len(ps) * cap
        factors = []
        for p in ps:
            line = (sc_in if p else sc_out)[p]
            factors.append(jnp.broadcast_to(line, (128, 128)).T[0:cap, 0:1])
        factor = jnp.concatenate(factors, 0)
        span = pl.ds(ps[0] * cap, m)

        def up(i, _):
            cols = pl.ds(pl.multiple_of(i * tile, tile), tile)
            a = jnp.zeros((m, tile), F32)
            b = jnp.zeros((m, tile), F32)
            for j in range(tps):
                x = rows[ps[0]:ps[0] + len(ps), j].reshape(m, DT)
                a = a + dot(x, eg[j * DT:(j + 1) * DT, cols])
                b = b + dot(x, eu[j * DT:(j + 1) * DT, cols])
            hid[span, cols] = (silu(a * factor) * (b * factor)).astype(BF16)
            return 0

        lax.fori_loop(start, stop, up, 0)

    def expert_down(gi, half):
        span = span_of(gi)
        whole = pl.ds(groups[gi][0] * cap, len(groups[gi]) * cap)

        def down(j):
            s2[j, whole] = dot(hid[whole, :], ed[:, pl.ds(pl.multiple_of(j * DT, DT), DT)]).astype(BF16)

        for i, y2 in enumerate((1 - yy, yy)):
            if i in half:
                down(y2 * 2 + 1 - core)
                send(s2.at[y2 * 2 + 1 - core, span], p2.at[i, span], r2_ss.at[gi, i], r2_rs.at[gi, i], {"tp": mate})
                down(y2 * 2 + core)

    def span_of(gi):
        away = [p for p in groups[gi] if p]
        return pl.ds(away[0] * cap, len(away) * cap)

    def scatter_sum(gi):
        span = span_of(gi)
        arrived(p2.at[0, span], r2_ss.at[gi, 0], r2_rs.at[gi, 0], {"tp": mate})
        q2[span] = (s2[across, span].astype(F32) + p2[0, span].astype(F32)).astype(BF16)

    def scatter_send(*ps):
        for p in ps:
            piece = pl.ds(p * cap, cap)
            send(q2.at[piece], z2.at[piece], q_ss.at[p], q_rs.at[p], {"tp": across})

    def mate_sum(gi):
        arrived(p2.at[1, span_of(gi)], r2_ss.at[gi, 1], r2_rs.at[gi, 1], {"tp": mate})

    def give_back(*ps):
        for p in ps:
            piece = pl.ds(p * cap, cap)
            arrived(z2.at[piece], q_ss.at[p], q_rs.at[p], {"tp": across})
            total = (s2[mt, piece].astype(F32) + p2[1, piece].astype(F32) + z2[piece].astype(F32)).astype(BF16)
            back[p] = total
            send(back.at[p], ret.at[piece], b_ss.at[p], b_rs.at[p], {"sp": peer(p)})

    def collect(gi):
        span = span_of(gi)
        for p in groups[gi]:
            if p:
                arrived(ret.at[pl.ds(p * cap, cap)], b_ss.at[p], b_rs.at[p], {"sp": peer(p)})
        total = hidden_ref[...]
        for k in range(2):
            weight = jnp.broadcast_to(weights_ref[k:k + 1, :], (R, R)).T[:, 0:1]
            chosen = lax.dot_general(
                sel[k, span], ret[span], (((0,), (0,)), ((), ())), preferred_element_type=F32)
            total = total + weight * chosen
        hidden_ref[...] = total

    forward_own(1)
    xs_across()
    forward_own(2)
    forward_across(1)
    xs_rest()
    forward_own(3)
    weights_here()
    all_here(0, 1)
    expert_up(0, 0, 2)
    forward_across(2)
    forward_own(4, 5)
    expert_up(0, 2, 4)
    expert_down(0, (0,))
    forward_own(6)
    expert_down(0, (1,))
    forward_across(3)
    shared()
    forward_own(7)
    all_here(2, 3)
    expert_up(1, 0, 2)
    forward_across(4)
    expert_up(1, 2, 4)
    forward_across(5)
    expert_down(1, (0, 1))
    scatter_sum(1)
    scatter_send(2, 3)
    scatter_sum(0)
    scatter_send(1)
    forward_across(6, 7)
    all_here(4, 5)
    expert_up(2, 0, 2)
    all_here(6, 7)
    expert_up(3)
    mate_sum(1)
    give_back(2)
    expert_down(3, (0, 1))
    scatter_sum(3)
    scatter_send(6, 7)
    give_back(3)
    expert_up(2, 2, 4)
    expert_down(2, (0, 1))
    mate_sum(0)
    give_back(1)
    mate_sum(3)
    scatter_sum(2)
    scatter_send(4, 5)
    shared_across()
    give_back(6, 7)
    mate_sum(2)
    give_back(4, 5)
    collect(0)
    collect(1)
    shared_end()
    collect(3)
    collect(2)
    out_ref[...] = hidden_ref[...].astype(BF16)
    for copy in sends:
        copy.wait_send()

    @pl.when(me < n - 1)
    def _():
        pltpu.make_async_remote_copy(
            src_ref=pool_ref.at[pl.ds(R - 16, 16)], dst_ref=halo_in,
            send_sem=halo_sem.at[0], recv_sem=halo_sem.at[1],
            device_id={"sp": following}, device_id_type=pl.DeviceIdType.MESH).wait_send()


def body(
    pool_input, doc_ids, residual, pool_gain, out_proj, norm_gain, routes, route_weights,
    expert_gate, expert_up, expert_down, shared_gate, shared_up, shared_down,
):
    n, tps = lax.axis_size("sp"), lax.axis_size("tp")
    R, C = pool_input.shape
    DT = residual.shape[1]
    FF, FS, D = expert_gate.shape[2], shared_gate.shape[1], expert_gate.shape[1]
    experts = expert_gate.shape[0] * n
    top = routes.shape[1]
    cap = tps * max(1, 2 * R * top // (experts * tps))
    groups = [[0, 1], [2, 3], [4, 5], [6, 7]]
    V, DMA = pltpu.VMEM, pltpu.SemaphoreType.DMA
    scratch = [
        V((R, C), BF16), V((1, R), jnp.int32), V((top, R), jnp.int32), V((top, R), F32),
        V((R, DT), BF16), V((1, C), F32), V((1, DT), F32), DMA((7,)),
        V((C, D), BF16), V((D, FF), BF16), V((D, FF), BF16), V((FF, D), BF16),
        V((D, FS), BF16), V((D, FS), BF16), V((FS, D), BF16), DMA((7,)),
        V((1, C + 256), F32), V((n, 1, C + 256), F32), V((16, C), BF16), DMA((n,)), DMA((n,)), DMA((2,)),
        V((tps, R, DT), BF16), V((2, R, DT), BF16), V((R, DT), BF16), V((R, DT), BF16), DMA((4,)), DMA((4,)),
        V((8, R), F32), V((tps, 8, R), F32), DMA((tps,)), DMA((tps,)),
        V((2, n * cap, R), BF16), V((n * cap, R), BF16), V((n, 1, 128), F32), V((n, 1, 128), F32), DMA((n,)), DMA((n,)),
        V((n, cap, DT), BF16), V((n, tps, cap, DT), BF16),
        DMA((n, 2)), DMA((n, 2)), DMA((n, 3)), DMA((n, 3)),
        V((R, DT), BF16), V((tps, R, DT), BF16), DMA((5,)), DMA((5,)),
        V((tps, R, DT), BF16), V((2, R, DT), BF16), V((R, DT), BF16), V((R, DT), BF16), DMA((3,)), DMA((3,)),
        V((n * cap, FF), BF16), V((tps, n * cap, DT), BF16), V((2, n * cap, DT), BF16),
        V((n * cap, DT), BF16), V((n * cap, DT), BF16), DMA((len(groups), 2)), DMA((len(groups), 2)), DMA((n,)), DMA((n,)),
        V((n, cap, DT), BF16), V((n * cap, DT), BF16), DMA((n,)), DMA((n,)),
        V((R, DT), F32),
    ]
    vm = pl.BlockSpec(memory_space=pltpu.VMEM)
    hb = pl.BlockSpec(memory_space=pltpu.HBM)
    return pl.pallas_call(
        functools.partial(layer_kernel, groups),
        out_shape=pltpu.VMEM((R, DT), BF16),
        in_specs=[hb] * 14,
        out_specs=vm,
        scratch_shapes=scratch,
        compiler_params=pltpu.CompilerParams(
            collective_id=0, has_side_effects=True, vmem_limit_bytes=60 * 2**20),
    )(pool_input, doc_ids.reshape(1, R), routes.T, route_weights.T, residual, pool_gain.reshape(1, C), norm_gain.reshape(1, DT),
      out_proj, expert_gate, expert_up, expert_down, shared_gate, shared_up, shared_down)


def one_kernel_fits(mesh):
    return mesh.shape["tp"] == 4 and mesh.shape["sp"] == 8


def solution(mesh):
    placed = (
        P("sp", "tp"),
        P("sp"),
        P("sp", "tp"),
        P("tp"),
        P("tp", None),
        P("tp"),
        P("sp", None),
        P("sp", None),
        P("sp", None, "tp"),
        P("sp", None, "tp"),
        P("sp", "tp", None),
        P(None, "tp"),
        P(None, "tp"),
        P("tp", None),
    )
    return jax.shard_map(
        body if one_kernel_fits(mesh) else plain_body, mesh=mesh, in_specs=placed, out_specs=P("sp", "tp"), check_vma=False)
```
